32 devices in a mesh: grp: 2 (over y), kv: 4 (over z), tp: 4 (over x, core).
Axes of the slice: x: 2, y: 2, z: 4, core: 2. Of those that a mesh axis runs over, the one named last changes fastest.
Arguments:
- tokens: bfloat16 [256, 4, 2048], P(('grp', 'kv'), None, 'tp'), parts along dimension 0, may hold values from -6 to 6
- in_gain: float32 [2048], replicated, may hold values from 0.1 to 1.9
- w_query: bfloat16 [2048, 1024], P('kv', 'tp'), may hold values from -0.125 to 0.125
- w_key: bfloat16 [2048, 1024], P('kv', 'tp'), may hold values from -0.125 to 0.125
- w_value: bfloat16 [2048, 1024], P('kv', 'tp'), may hold values from -0.125 to 0.125
- w_gate: bfloat16 [2048, 1024], P('kv', 'tp'), may hold values from -0.125 to 0.125
- w_beta: bfloat16 [2048, 16], replicated, may hold values from -0.125 to 0.125
- w_decay: bfloat16 [2048, 16], replicated, may hold values from -0.125 to 0.125
- decay_base: float32 [16], P('tp'), may hold values from 0.05 to 1
- out_gain: float32 [64], replicated, may hold values from 0.1 to 1.9
- w_out: bfloat16 [1024, 2048], P('tp', 'kv'), may hold values from -0.1875 to 0.1875
- state: float32 [256, 64, 1024], P(('grp', 'kv'), None, 'tp'), parts along dimension 0, may hold values from -0.8 to 0.8
- prev_keys: bfloat16 [256, 4, 1024], P(('grp', 'kv'), None, 'tp'), parts along dimension 0, may hold values from -6 to 6
- prev_values: bfloat16 [256, 4, 1024], P(('grp', 'kv'), None, 'tp'), parts along dimension 0, may hold values from -6 to 6
- prev_beta: float32 [256, 4, 16], P(('grp', 'kv'), None, 'tp'), parts along dimension 0, may hold values from -6 to 6
- prev_decay: float32 [256, 4, 16], P(('grp', 'kv'), None, 'tp'), parts along dimension 0, may hold values from -1 to -0.02
- accepted: int32 [256], P(('grp', 'kv')), parts along dimension 0, may hold values from 0 to 4
Outputs:
- mixed: bfloat16 [256, 4, 2048], P(('grp', 'kv'), None, 'tp'), parts along dimension 0
- new_state: float32 [256, 64, 1024], P(('grp', 'kv'), None, 'tp'), parts along dimension 0
The draws below stay inside these ranges and needn't reach their ends.
There are 2 independent parts, one for each index of `grp`. The reference program is written for one: setup_inputs(seed, part) draws one part's arguments, and reference() takes and returns one part's arrays. A program takes and returns all parts, laid end to end along the dimension named above; an argument that names none is the same for every part. Nothing has to cross between parts.
All inputs are finite; a program needn't handle non-finite values.
Results may differ from the reference program's by a relative error of at most 0.012.
Values may be sent and summed in bfloat16 or wider, within the bound.
No kernel may reach another device: no remote copies, remote signals or barrier semaphores. Data moves between devices by JAX's collectives and lax.ppermute only.
A program may use at most 128 MiB of HBM per device.

```python
import math
import jax
import jax.numpy as jnp
from jax import lax

D = 2048
HEADS = 16
HD = 64
P_SIZE = 4
SEQ_DEV = 32
SEQS = 128
N_KV = 4


def plant(entries, rng, least, top_value):
    spot = [jax.random.randint(jax.random.fold_in(rng, axis), (), 0, length) for axis, length in enumerate(entries.shape)]
    widest = entries.shape.index(max(entries.shape))
    neighbour = spot[:widest] + [(spot[widest] + 1) % entries.shape[widest]] + spot[widest + 1:]
    return entries.at[tuple(spot)].set(least).at[tuple(neighbour)].set(top_value)


def shard_levels(stream_key, shape, cuts, smallest, high):
    gain = 1.0
    for axis_at, shards_of in cuts:
        draws = jax.random.uniform(jax.random.fold_in(jax.random.fold_in(stream_key, 6), axis_at), (shards_of,), jnp.float32, smallest / len(cuts), high / len(cuts))
        gain = gain * jnp.repeat(jnp.exp(draws), shape[axis_at] // shards_of).reshape((-1,) + (1,) * (len(shape) - 1 - axis_at))
    return gain


def centred(own_key, dims, scale, limit, split=(), kind=jnp.bfloat16):
    entries = scale * jax.random.normal(own_key, dims, jnp.float32)
    if split:
        entries = entries * shard_levels(own_key, dims, split, -0.22, 0.18)
    return jnp.clip(entries, -limit, limit).astype(kind)


def setup_inputs(seed: int = 0, part: int = 0) -> dict:
    splits = jax.random.split(jax.random.key(seed), 18)
    part_keys = jax.random.split(jax.random.fold_in(splits[17], part), 18)
    return {
        "tokens": centred(part_keys[0], (SEQS, P_SIZE, D), 1.0, 6.0, ((0, 4), (2, 4))),
        "in_gain": jnp.clip(1.0 + 0.18 * jax.random.normal(splits[1], (D,), jnp.float32), 0.1, 1.9),
        "w_query": centred(splits[2], (D, HEADS * HD), D ** -0.5, 0.125, ((0, 4), (1, 4))),
        "w_key": centred(splits[3], (D, HEADS * HD), D ** -0.5, 0.125, ((0, 4), (1, 4))),
        "w_value": centred(splits[4], (D, HEADS * HD), D ** -0.5, 0.125, ((0, 4), (1, 4))),
        "w_gate": centred(splits[5], (D, HEADS * HD), D ** -0.5, 0.125, ((0, 4), (1, 4))),
        "w_beta": centred(splits[6], (D, HEADS), D ** -0.5, 0.125),
        "w_decay": centred(splits[7], (D, HEADS), D ** -0.5, 0.125),
        "decay_base": jnp.clip(jnp.exp(math.log(1.0) - 2.9957323 * jax.random.uniform(splits[8], (HEADS,), jnp.float32) ** shard_levels(splits[8], (HEADS,), ((0, 4),), -0.2, 0.2)), 0.05, 1.0),
        "out_gain": jnp.clip(1.0 + 0.18 * jax.random.normal(splits[9], (HD,), jnp.float32), 0.1, 1.9),
        "w_out": centred(splits[10], (HEADS * HD, D), (HEADS * HD) ** -0.5, 0.1875, ((0, 4), (1, 4))),
        "state": centred(part_keys[11], (SEQS, HD, HEADS * HD), 0.1, 0.8, ((0, 4), (2, 4)), jnp.float32),
        "prev_keys": centred(part_keys[12], (SEQS, P_SIZE, HEADS * HD), 1.0, 6.0, ((0, 4), (2, 4))),
        "prev_values": centred(part_keys[13], (SEQS, P_SIZE, HEADS * HD), 1.0, 6.0, ((0, 4), (2, 4))),
        "prev_beta": centred(part_keys[14], (SEQS, P_SIZE, HEADS), 1.5, 6.0, ((0, 4), (2, 4)), jnp.float32),
        "prev_decay": jnp.clip(-1.0 + 0.98 * jax.random.uniform(part_keys[15], (SEQS, P_SIZE, HEADS), jnp.float32) ** shard_levels(part_keys[15], (SEQS, P_SIZE, HEADS), ((0, 4), (2, 4)), -0.2, 0.2), -1.0, -0.02),
        "accepted": plant(jax.random.randint(part_keys[16], (SEQS,), 0, P_SIZE + 1), jax.random.fold_in(part_keys[16], 1), 0, P_SIZE).astype(jnp.int32),
    }


EPS = 1e-06

def normalize_rows(vector):
    return vector * lax.rsqrt(lax.optimization_barrier(jnp.sum(vector * vector, -1, keepdims=True)) + EPS)

def delta_block(saved, queries, keys_in, values_in, strength, log_decay):
    highest = lax.Precision.HIGHEST
    steps_len = queries.shape[1]
    cumul = jnp.transpose(jnp.cumsum(log_decay, axis=1), (0, 2, 1))
    q_heads = jnp.transpose(queries, (0, 2, 1, 3))
    k_heads = jnp.transpose(keys_in, (0, 2, 1, 3))
    v_heads = jnp.transpose(values_in, (0, 2, 1, 3))
    weight_t = jnp.transpose(strength, (0, 2, 1))
    spread = cumul[..., :, None] - cumul[..., None, :]
    order = jnp.arange(steps_len)
    inside = order[:, None] >= order[None, :]
    below = order[:, None] > order[None, :]
    dec_incl = jnp.where(inside, jnp.exp(jnp.where(inside, spread, 0.0)), 0.0)
    dec_strict = jnp.where(below, dec_incl, 0.0)
    lower_mat = weight_t[..., :, None] * jnp.einsum('bhik,bhjk->bhij', k_heads, k_heads, precision=highest) * dec_strict
    growth = jnp.exp(cumul)
    rhs_all = jnp.concatenate([weight_t[..., None] * v_heads, (weight_t * growth)[..., None] * k_heads], axis=-1)
    solved = []
    for row_index in range(steps_len):
        current = rhs_all[:, :, row_index]
        for col_index in range(row_index):
            current = current - lower_mat[:, :, row_index, col_index, None] * solved[col_index]
        solved.append(current)
    solution = jnp.stack(solved, axis=2)
    value_size = v_heads.shape[-1]
    update = solution[..., :value_size] - jnp.einsum('bhpk,bhkv->bhpv', solution[..., value_size:], saved, precision=highest)
    scores = jnp.einsum('bhik,bhjk->bhij', q_heads, k_heads, precision=highest) * dec_incl
    output = jnp.einsum('bhpk,bhkv->bhpv', growth[..., None] * q_heads, saved, precision=highest) + jnp.einsum('bhij,bhjv->bhiv', scores, update, precision=highest)
    tail = jnp.exp(cumul[..., -1:] - cumul)[..., None] * k_heads
    renewed = jnp.exp(cumul[..., -1])[..., None, None] * saved + jnp.einsum('bhpk,bhpv->bhkv', tail, update, precision=highest)
    return (jnp.transpose(output, (0, 2, 1, 3)), renewed)

def reference(tokens, in_gain, w_query, w_key, w_value, w_gate, w_beta, w_decay, decay_base, out_gain, w_out, state, prev_keys, prev_values, prev_beta, prev_decay, accepted):
    rows = SEQS * P_SIZE
    wide = tokens.astype(jnp.float32)
    normed = (wide * lax.rsqrt(lax.optimization_barrier(jnp.mean(wide * wide, -1, keepdims=True)) + EPS) * in_gain).astype(jnp.bfloat16)
    flat = normed.reshape(rows, D)
    shape4 = (SEQS, P_SIZE, HEADS, HD)
    query = normalize_rows(jnp.dot(flat, w_query, preferred_element_type=jnp.float32).reshape(shape4)) * HD ** (-0.5)
    key_vec = normalize_rows(jnp.dot(flat, w_key, preferred_element_type=jnp.float32).reshape(shape4))
    value_vec = jnp.dot(flat, w_value, preferred_element_type=jnp.float32).reshape(shape4)
    gate = jnp.dot(flat, w_gate, preferred_element_type=jnp.float32).reshape(shape4)
    strength = jax.nn.sigmoid(jnp.dot(flat, w_beta, preferred_element_type=jnp.float32)).reshape(SEQS, P_SIZE, HEADS)
    log_decay = (-decay_base * jax.nn.softplus(jnp.dot(flat, w_decay, preferred_element_type=jnp.float32))).reshape(SEQS, P_SIZE, HEADS)
    live = (jnp.arange(P_SIZE, dtype=jnp.int32)[None, :] < accepted[:, None]).astype(jnp.float32)
    prev_strength = jax.nn.sigmoid(prev_beta) * live[..., None]
    prev_log = prev_decay * live[..., None]
    prev_k = normalize_rows(prev_keys.astype(jnp.float32).reshape(shape4))
    prev_v = prev_values.astype(jnp.float32).reshape(shape4)
    saved = jnp.transpose(state.reshape(SEQS, HD, HEADS, HD), (0, 2, 1, 3))

    def per_block(inputs):
        held, pk_in, pv_in, pb_in, pg_in, qu_in, ke_in, va_in, st_in, lg_in = inputs
        committed = delta_block(held, pk_in, pk_in, pv_in, pb_in, pg_in)[1]
        output = delta_block(committed, qu_in, ke_in, va_in, st_in, lg_in)[0]
        return (output, committed)
    pieces = (saved, prev_k, prev_v, prev_strength, prev_log, query, key_vec, value_vec, strength, log_decay)
    blocked = tuple((array.reshape((N_KV, SEQ_DEV) + array.shape[1:]) for array in pieces))
    output, committed = lax.map(per_block, blocked)
    output = output.reshape(shape4)
    committed = committed.reshape(SEQS, HEADS, HD, HD)
    gated = (output * lax.rsqrt(lax.optimization_barrier(jnp.mean(output * output, -1, keepdims=True)) + EPS) * out_gain * jax.nn.silu(gate)).astype(jnp.bfloat16).reshape(rows, HEADS * HD)
    mixed = jnp.dot(gated, w_out, preferred_element_type=jnp.float32).astype(jnp.bfloat16).reshape(SEQS, P_SIZE, D)
    new_state = jnp.transpose(committed, (0, 2, 1, 3)).reshape(SEQS, HD, HEADS * HD)
    return (mixed, new_state)
```

```python
import functools

import jax
import jax.numpy as jnp
from jax import lax
from jax.experimental import pallas as pl
from jax.experimental.pallas import tpu as pltpu
from jax.sharding import PartitionSpec as P

EPS = 1e-06
CHUNKS = 1
F32 = jnp.float32
BF16 = jnp.bfloat16
VMEM = pltpu.VMEM
SMEM = pltpu.SMEM
ANY = pl.ANY


def whole(space=VMEM):
    return pl.BlockSpec(memory_space=space)


def dot(a, b, contract=((1,), (0,)), precision=None):
    return lax.dot_general(
        a, b, (contract, ((), ())), precision=precision, preferred_element_type=F32
    )


def head_ones(width, size):
    row = lax.broadcasted_iota(jnp.int32, (width, width), 0) // size
    col = lax.broadcasted_iota(jnp.int32, (width, width), 1) // size
    return jnp.where(row == col, 1.0, 0.0).astype(BF16)


def head_sum(values, ones):
    high = values.astype(BF16)
    low = (values - high.astype(F32)).astype(BF16)
    return dot(high, ones) + dot(low, ones)


def head_mask(first, group, steps, width, size):
    sub = lax.broadcasted_iota(jnp.int32, (group * steps, width), 0) // steps + first
    lane = lax.broadcasted_iota(jnp.int32, (group * steps, width), 1) // size
    return sub == lane


def prep_kernel(steps, place, tok_ref, gain_ref, wt_ref, *out_refs):
    chunk_refs, stat_ref = out_refs[:-1], out_refs[-1]
    seqs = tok_ref.shape[0]
    each = seqs // len(chunk_refs)
    raw = [tok_ref[:, t, :].astype(F32) for t in range(steps)]
    gain = gain_ref[...]
    scaled = [(x * gain).astype(BF16) for x in raw]
    for c, ref in enumerate(chunk_refs):
        for t in range(steps):
            ref[t * each : (t + 1) * each, :] = scaled[t][c * each : (c + 1) * each]
    full = jnp.concatenate(scaled, 0)
    logits = dot(wt_ref[...], full, ((1,), (1,)))
    square = jnp.concatenate([x * x for x in raw], 0)
    ones = jnp.ones((8, square.shape[1]), F32)
    total = dot(ones, square, ((1,), (1,)), lax.Precision.HIGHEST)
    count = logits.shape[0]
    stat_ref[0:count, :] = logits
    stat_ref[count : count + 8, :] = total


def prepare(tokens, in_gain, w_beta, w_decay, place, n_tp, chunks):
    seqs, steps, local = tokens.shape
    heads_all = w_beta.shape[1]
    wt = jnp.concatenate([w_beta, w_decay], 1).T
    each = seqs // chunks
    shapes = [jax.ShapeDtypeStruct((steps * each, local), BF16) for _ in range(chunks)]
    shapes.append(jax.ShapeDtypeStruct((2 * heads_all + 8, seqs * steps), F32))
    grid = pltpu.PrefetchScalarGridSpec(
        num_scalar_prefetch=1,
        grid=(1,),
        in_specs=[
            pl.BlockSpec((seqs, steps, local), lambda i, p: (0, 0, 0)),
            pl.BlockSpec((1, local), lambda i, p: (0, p[2])),
            pl.BlockSpec((2 * heads_all, local), lambda i, p: (0, p[2])),
        ],
        out_specs=[pl.BlockSpec(s.shape, lambda i, p: (0, 0)) for s in shapes],
    )
    out = pl.pallas_call(
        functools.partial(prep_kernel, steps), out_shape=shapes, grid_spec=grid, name="prep"
    )(place, tokens, in_gain.reshape(1, -1), wt)
    return out[:-1], out[-1]


def project_kernel(count, x_ref, *refs):
    weights, outs = refs[:count], refs[count:]
    width = weights[0].shape[1]
    order = list(range(1, len(outs))) + [0]
    for d in order:
        for w in range(count):
            outs[d][:, w * width : (w + 1) * width] = dot(x_ref[d], weights[w][...]).astype(
                outs[d].dtype
            )


def project(x, weights):
    owners, rows, _ = x.shape
    width = weights[0].shape[1] * len(weights)
    flops = 2 * x.size * width
    return pl.pallas_call(
        functools.partial(project_kernel, len(weights)),
        out_shape=[
            jax.ShapeDtypeStruct((rows, width), F32 if d == 0 else BF16) for d in range(owners)
        ],
        in_specs=[whole()] * (1 + len(weights)),
        out_specs=[whole()] * owners,
        cost_estimate=pl.CostEstimate(flops=flops, bytes_accessed=4 * x.size, transcendentals=0),
        name="project",
    )(x, *weights)


def spread_heads(ref, value, offset, stride, seqs, heads, steps, size, t):
    for h in range(heads):
        tile, lane = divmod(h * size, 128)
        part = value[:, tile * 128 : (tile + 1) * 128]
        if lane:
            part = pltpu.roll(part, 128 - lane, 1)
        ref[pl.ds(offset + h * steps + t, seqs, stride=stride), :] = part


def put_rows(ref, start, count, value, stride=None):
    for m in range(ref.shape[0]):
        ref[m, pl.ds(start, count, stride=stride), :] = value[:, m * 128 : (m + 1) * 128]


def get_rows(ref, start, count, stride=None):
    return jnp.concatenate(
        [ref[m, pl.ds(start, count, stride=stride), :] for m in range(ref.shape[0])], 1
    )


def own_heads(product, masks, group, steps):
    tile = group * steps
    total = None
    for m, mask in enumerate(masks):
        part = jnp.where(mask, product[m * tile : (m + 1) * tile], 0.0)
        total = part if total is None else total + part
    shift = steps
    acc = total
    for _ in range(group - 1):
        acc = acc + pltpu.roll(total, shift, 0)
        shift += steps
    return acc


def catch_kernel(
    steps, size, s0_ref, k_ref, v_ref, b_ref, d_ref, a_ref, out_ref, kscr, pscr, uscr, gscr
):
    seqs, _, width = s0_ref.shape
    heads = width // size
    group = 8 // steps
    ones = head_ones(width, size)
    masks = [head_mask(g * group, group, steps, width, size) for g in range(heads // group)]
    pick = jnp.where(
        lax.broadcasted_iota(jnp.int32, (heads, width), 0)
        == lax.broadcasted_iota(jnp.int32, (heads, width), 1) // size,
        1.0,
        0.0,
    )
    keys = [k_ref[:, t, :].astype(F32) for t in range(steps)]
    for t in range(steps):
        spread_heads(kscr, keys[t], 0, heads * steps, seqs, heads, steps, size, t)
    pairs = [(t, r) for t in range(steps) for r in range(t + 1)]
    sums = head_sum(jnp.concatenate([keys[t] * keys[r] for t, r in pairs], 0), ones)
    raw = {p: sums[i * seqs : (i + 1) * seqs] for i, p in enumerate(pairs)}
    inv = [lax.rsqrt(raw[t, t] + EPS) for t in range(steps)]

    def read(s, carry):
        kb = kscr[pl.ds(s * heads * steps, heads * steps), :][:, :size].astype(BF16)
        seen = own_heads(dot(kb, s0_ref[s].astype(BF16)), masks, group, steps)
        put_rows(pscr, s * 8, 8, seen)
        return carry

    lax.fori_loop(0, seqs, read, 0, unroll=8)
    live = [jnp.where(a_ref[...] > t, 1.0, 0.0) for t in range(steps)]
    highest = lax.Precision.HIGHEST
    cumul, solved = [], []
    for t in range(steps):
        log = dot(d_ref[:, t, :], pick, precision=highest) * live[t]
        strength = jax.nn.sigmoid(dot(b_ref[:, t, :], pick, precision=highest)) * live[t]
        cumul.append(log if t == 0 else cumul[-1] + log)
        seen = get_rows(pscr, t, seqs, 8) * inv[t]
        rest = v_ref[:, t, :].astype(F32) - jnp.exp(cumul[t]) * seen
        for r in range(t):
            rest = rest - jnp.exp(cumul[t] - cumul[r]) * (raw[t, r] * inv[t] * inv[r]) * solved[r]
        solved.append(strength * rest)
    for t in range(steps):
        add = jnp.exp(cumul[-1] - cumul[t]) * inv[t] * solved[t]
        for g in range(group):
            put_rows(uscr, g * steps + t, seqs, add, 8)
    gscr[...] = jnp.exp(cumul[-1])

    def write(s, carry):
        ub = get_rows(uscr, s * 8, 8)
        wide = jnp.concatenate([jnp.where(m, ub, 0.0) for m in masks], 0).astype(BF16)
        kb = kscr[pl.ds(s * heads * steps, heads * steps), :][:, :size].astype(BF16)
        out_ref[s] = gscr[pl.ds(s, 1), :] * s0_ref[s] + dot(kb, wide, ((0,), (0,)))
        return carry

    lax.fori_loop(0, seqs, write, 0, unroll=8)


def catch_up(state, prev_keys, prev_values, prev_beta, prev_decay, accepted):
    seqs, size, width = state.shape
    steps = prev_keys.shape[1]
    heads = width // size
    return pl.pallas_call(
        functools.partial(catch_kernel, steps, size),
        out_shape=jax.ShapeDtypeStruct(state.shape, F32),
        in_specs=[whole()] * 6,
        out_specs=whole(),
        scratch_shapes=[
            VMEM((seqs * heads * steps, 128), F32),
            VMEM((width // 128, seqs * 8, 128), F32),
            VMEM((width // 128, seqs * 8, 128), F32),
            VMEM((seqs, width), F32),
        ],
        cost_estimate=pl.CostEstimate(
            flops=seqs * 4000000, bytes_accessed=8 * state.size, transcendentals=0
        ),
        name="catch_up",
    )(state, prev_keys, prev_values, prev_beta, prev_decay, accepted.reshape(-1, 1))


def propose_kernel(
    dims, parts, blocks, place, stat_ref, base_ref, gain_ref, s_ref, *refs
):
    steps, size, features, heads_all = dims
    part_refs, refs = refs[:parts], refs[parts:]
    block_refs, refs = refs[: len(blocks)], refs[len(blocks) :]
    out_refs, refs = refs[:-4], refs[-4:]
    kscr, pscr, wo, sems = refs
    seqs, _, width = s_ref.shape
    heads = width // size
    group = 8 // steps
    kv, tp = place[1], place[2]

    copies = []
    for i, (place_of, ref) in enumerate(zip(blocks, block_refs)):
        target = place_of(place, wo)
        copies.append(pltpu.make_async_copy(ref, target, sems.at[i]))
        copies[-1].start()

    ones = head_ones(width, size)
    masks = [head_mask(g * group, group, steps, width, size) for g in range(heads // group)]
    rows = seqs * steps
    stat = stat_ref[...]
    count = stat.shape[0]
    src = lax.broadcasted_iota(jnp.int32, (count, width), 0)
    head = lax.broadcasted_iota(jnp.int32, (count, width), 1) // size + tp * heads
    highest = lax.Precision.HIGHEST
    flat = stat.T

    def take(row):
        return dot(flat, jnp.where(src == row, 1.0, 0.0), precision=highest)

    scale = lax.rsqrt(take(2 * heads_all) / features + EPS)
    strength = jax.nn.sigmoid(scale * take(head))
    rate = scale * take(heads_all + head)
    log = -base_ref[...] * (jnp.maximum(rate, 0.0) + jnp.log1p(jnp.exp(-jnp.abs(rate))))

    def column(w):
        lanes = slice(w * width, (w + 1) * width)
        total = part_refs[0][:, lanes].astype(F32)
        for ref in part_refs[1:]:
            total = total + ref[:, lanes].astype(F32)
        return total * scale

    query, key = column(0), column(1)
    squares = head_sum(jnp.concatenate([query * query, key * key], 0), ones)
    query = query * (lax.rsqrt(squares[:rows] + EPS) * size ** (-0.5))
    key = key * lax.rsqrt(squares[rows:] + EPS)

    def at(array, t):
        return array[t * seqs : (t + 1) * seqs]

    stride = 2 * heads * steps
    for t in range(steps):
        spread_heads(kscr, at(query, t), 0, stride, seqs, heads, steps, size, t)
        spread_heads(kscr, at(key, t), heads * steps, stride, seqs, heads, steps, size, t)
    below = [(t, r) for t in range(steps) for r in range(t)]
    inside = [(t, r) for t in range(steps) for r in range(t + 1)]
    products = [at(key, t) * at(key, r) for t, r in below]
    products += [at(query, t) * at(key, r) for t, r in inside]
    sums = head_sum(jnp.concatenate(products, 0), ones)
    k_k = {p: at(sums, i) for i, p in enumerate(below)}
    q_k = {p: at(sums, len(below) + i) for i, p in enumerate(inside)}
    upper = lax.broadcasted_iota(jnp.int32, (8, width), 0) < steps

    def read(s, carry):
        vectors = kscr[pl.ds(s * stride, stride), :][:, :size].astype(BF16)
        seen = dot(vectors, s_ref[s].astype(BF16))
        half = heads * steps
        from_query = own_heads(seen[:half], masks, group, steps)
        from_key = own_heads(seen[half:], masks, group, steps)
        put_rows(pscr, s * 8, 8, jnp.where(upper, from_query, from_key))
        return carry

    lax.fori_loop(0, seqs, read, 0, unroll=8)
    value, gate = column(2), column(3)
    cumul, solved, outs = [], [], []
    for t in range(steps):
        cumul.append(at(log, t) if t == 0 else cumul[-1] + at(log, t))
        grown = jnp.exp(cumul[t])
        rest = at(value, t) - grown * get_rows(pscr, steps + t, seqs, 8)
        out = grown * get_rows(pscr, t, seqs, 8)
        for r in range(t):
            decay = jnp.exp(cumul[t] - cumul[r])
            rest = rest - decay * k_k[t, r] * solved[r]
            out = out + decay * q_k[t, r] * solved[r]
        solved.append(at(strength, t) * rest)
        outs.append(out + q_k[t, t] * solved[t])
    output = jnp.concatenate(outs, 0)
    mean = head_sum(output * output, ones) * (1.0 / size)
    gated = output * lax.rsqrt(mean + EPS) * gain_ref[...] * (gate / (1.0 + jnp.exp(-gate)))
    gated = gated.astype(BF16)
    if not blocks:
        out_refs[0][...] = gated
        return
    for copy in copies:
        copy.wait()
    n = wo.shape[0]
    for s in list(range(1, n)) + [0]:
        out_refs[s][...] = dot(gated, wo[lax.rem(tp + s, n)]).astype(out_refs[s].dtype)


def propose(place, stat, base, gain, state, parts, blocks, block_arrays, n_tp, dims, seqs, first):
    steps, size = dims[0], dims[1]
    width = state.shape[2]
    heads = width // size
    rows = seqs * steps
    if blocks:
        share = dims[2] // n_tp
        shapes = [
            jax.ShapeDtypeStruct((rows, share), F32 if s == 0 else BF16) for s in range(n_tp)
        ]
        wo = VMEM((n_tp, width, share), BF16)
    else:
        shapes = [jax.ShapeDtypeStruct((rows, width), BF16)]
        wo = VMEM((8, 128), F32)
    grid = pltpu.PrefetchScalarGridSpec(
        num_scalar_prefetch=1,
        grid=(1,),
        in_specs=[
            pl.BlockSpec(stat.shape, lambda i, p: (0, 0)),
            pl.BlockSpec((1, width), lambda i, p: (0, 0)),
            pl.BlockSpec((1, width), lambda i, p: (0, 0)),
            pl.BlockSpec((seqs,) + state.shape[1:], lambda i, p: (first, 0, 0)),
        ]
        + [pl.BlockSpec(a.shape, lambda i, p: (0, 0)) for a in parts]
        + [whole(ANY)] * len(blocks),
        out_specs=[pl.BlockSpec(s.shape, lambda i, p: (0, 0)) for s in shapes],
        scratch_shapes=[
            VMEM((seqs * 2 * heads * steps, 128), F32),
            VMEM((width // 128, seqs * 8, 128), F32),
            wo,
            pltpu.SemaphoreType.DMA((max(1, len(blocks)),)),
        ],
    )
    return pl.pallas_call(
        functools.partial(propose_kernel, dims, len(parts), blocks),
        out_shape=shapes,
        grid_spec=grid,
        cost_estimate=pl.CostEstimate(
            flops=seqs * 4000000, bytes_accessed=4 * state.size, transcendentals=0
        ),
        name="propose",
    )(place, stat, base, gain, state, *parts, *block_arrays)


def finish_kernel(steps, chunks, *refs):
    ins, out_ref = refs[:-1], refs[-1]
    per = len(ins) // chunks
    each = out_ref.shape[0] // chunks
    for c in range(chunks):
        total = ins[c * per][...].astype(F32)
        for ref in ins[c * per + 1 : (c + 1) * per]:
            total = total + ref[...].astype(F32)
        for t in range(steps):
            out_ref[c * each : (c + 1) * each, t, :] = total[t * each : (t + 1) * each].astype(
                out_ref.dtype
            )


def finish(pieces, seqs, steps):
    chunks = len(pieces)
    flat = [a for piece in pieces for a in piece]
    return pl.pallas_call(
        functools.partial(finish_kernel, steps, chunks),
        out_shape=jax.ShapeDtypeStruct((seqs, steps, flat[0].shape[1]), BF16),
        in_specs=[whole()] * len(flat),
        out_specs=whole(),
        name="finish",
    )(*flat)


def body(
    sizes,
    tokens,
    in_gain,
    w_query,
    w_key,
    w_value,
    w_gate,
    w_beta,
    w_decay,
    decay_base,
    out_gain,
    w_out,
    state,
    prev_keys,
    prev_values,
    prev_beta,
    prev_decay,
    accepted,
):
    n_grp, n_kv, n_tp = sizes
    seqs, steps, local = tokens.shape
    heads = decay_base.shape[0]
    size = out_gain.shape[0]
    features = in_gain.shape[0]
    heads_all = w_beta.shape[1]
    dims = (steps, size, features, heads_all)
    square = n_kv == n_tp and n_grp == 2
    chunks = CHUNKS if square else 1
    each = seqs // chunks
    place = jnp.stack([lax.axis_index("grp"), lax.axis_index("kv"), lax.axis_index("tp")])
    place = place.astype(jnp.int32)
    base = jnp.repeat(decay_base, size).reshape(1, -1)
    gain = jnp.tile(out_gain, heads).reshape(1, -1)
    weights = (w_query, w_key, w_value, w_gate)

    scaled, stat = prepare(tokens, in_gain, w_beta, w_decay, place, n_tp, chunks)

    def ring(n, s):
        return [(i, (i + s) % n) for i in range(n)]

    if square:
        n = n_kv
        turn = [(k * n + t, t * n + (k - t) % n) for k in range(n) for t in range(n)]
        turned = [lax.ppermute(x, ("kv", "tp"), turn) for x in scaled]
        half = w_out.shape[0] // n_grp
        mine = lax.dynamic_slice_in_dim(w_out, place[0] * half, half, 0)
        blocks = [lambda p, wo: wo.at[p[1]]]
        arrays = [w_out]
        for s in range(1, n):
            got = lax.ppermute(mine, "kv", ring(n, s))
            other = lax.ppermute(got, "grp", ring(n_grp, 1))
            arrays += [got, other]
            for g in range(n_grp):

                def target(p, wo, s=s, g=g):
                    row = lax.rem(p[0] + g, n_grp) * half
                    return wo.at[lax.rem(p[1] - s + n, n), pl.ds(pl.multiple_of(row, half), half), :]

                blocks.append(target)
        stat_all = jnp.sum(lax.all_gather(stat, "tp"), 0)
        parts = []
        for x in turned:
            mine_parts = project(lax.all_gather(x, "tp"), weights)
            parts.append(
                [mine_parts[0]]
                + [lax.ppermute(mine_parts[d], "kv", ring(n, d)) for d in range(1, n)]
            )
    else:
        blocks, arrays = [], []
        stat_all = jnp.sum(lax.all_gather(stat, "tp"), 0)
        x = lax.all_gather(scaled[0], "tp", axis=1, tiled=True)
        parts = [
            [
                jnp.concatenate(
                    [
                        jnp.dot(
                            x,
                            lax.all_gather(w, "kv", axis=0, tiled=True),
                            preferred_element_type=F32,
                        )
                        for w in weights
                    ],
                    1,
                )
            ]
        ]

    new_state = catch_up(state, prev_keys, prev_values, prev_beta, prev_decay, accepted)
    by_step = stat_all.reshape(stat_all.shape[0], steps, seqs)
    pieces = []
    for c in range(chunks):
        own = by_step[:, :, c * each : (c + 1) * each].reshape(stat_all.shape[0], -1)
        out = propose(
            place, own, base, gain, new_state, parts[c], blocks, arrays, n_tp, dims, each, c
        )
        if square:
            pieces.append(
                [out[0]] + [lax.ppermute(out[s], "tp", ring(n_tp, s)) for s in range(1, n_tp)]
            )
        else:
            full = lax.all_gather(w_out, "kv", axis=1, tiled=True)
            terms = jnp.dot(out[0], full, preferred_element_type=F32).astype(BF16)
            pieces.append([lax.psum_scatter(terms, "tp", scatter_dimension=1, tiled=True)])
    return finish(pieces, seqs, steps), new_state


def solution(mesh):
    rows = P(("grp", "kv"), None, "tp")
    matrix = P("kv", "tp")
    placed = (
        rows,
        P(),
        matrix,
        matrix,
        matrix,
        matrix,
        P(),
        P(),
        P("tp"),
        P(),
        P("tp", "kv"),
        rows,
        rows,
        rows,
        rows,
        rows,
        P(("grp", "kv")),
    )
    sizes = (mesh.shape["grp"], mesh.shape["kv"], mesh.shape["tp"])
    return jax.shard_map(
        functools.partial(body, sizes),
        mesh=mesh,
        in_specs=placed,
        out_specs=(rows, rows),
        check_vma=False,
    )
```

```python
import functools

import jax
import jax.numpy as jnp
from jax import lax
from jax.experimental import pallas as pl
from jax.experimental.pallas import tpu as pltpu
from jax.sharding import PartitionSpec as P

EPS = 1e-06
CHUNKS = 1
F32 = jnp.float32
BF16 = jnp.bfloat16
VMEM = pltpu.VMEM
HBM = pltpu.HBM


def whole(space=VMEM):
    return pl.BlockSpec(memory_space=space)


def fetch(sources, targets, sems):
    copies = [
        pltpu.make_async_copy(source, target, sems.at[i])
        for i, (source, target) in enumerate(zip(sources, targets))
    ]
    for copy in copies:
        copy.start()
    return copies


def like(array):
    return VMEM(array.shape, array.dtype)


def limit(mebibytes):
    return pltpu.CompilerParams(vmem_limit_bytes=mebibytes << 20)


def dot(a, b, contract=((1,), (0,)), precision=None):
    return lax.dot_general(
        a, b, (contract, ((), ())), precision=precision, preferred_element_type=F32
    )


def head_ones(width, size):
    row = lax.broadcasted_iota(jnp.int32, (width, width), 0) // size
    col = lax.broadcasted_iota(jnp.int32, (width, width), 1) // size
    return jnp.where(row == col, 1.0, 0.0).astype(BF16)


def head_sum(values, ones):
    high = values.astype(BF16)
    low = (values - high.astype(F32)).astype(BF16)
    return dot(high, ones) + dot(low, ones)


def head_mask(first, group, steps, width, size):
    sub = lax.broadcasted_iota(jnp.int32, (group * steps, width), 0) // steps + first
    lane = lax.broadcasted_iota(jnp.int32, (group * steps, width), 1) // size
    return sub == lane


def block_of(axis, size):
    return pl.ds(pl.multiple_of(lax.axis_index(axis) * size, size), size)


def statistics(steps, tok_ref, gain_ref, beta_ref, decay_ref, stat_ref):
    raw = jnp.concatenate([tok_ref[:, t, :].astype(F32) for t in range(steps)], 0)
    scaled = (raw * gain_ref[...]).astype(BF16)
    count = beta_ref.shape[0]
    stat_ref[:count, :] = dot(beta_ref[...], scaled, ((1,), (1,)))
    stat_ref[count : 2 * count, :] = dot(decay_ref[...], scaled, ((1,), (1,)))
    ones = jnp.ones((8, raw.shape[1]), F32)
    total = dot(ones, raw * raw, ((1,), (1,)), lax.Precision.HIGHEST)
    stat_ref[2 * count : 2 * count + 8, :] = total


def project_kernel(chunks, x_ref, gain_ref, weight_ref, *outs):
    owners, seqs, steps, _ = x_ref.shape
    each = seqs // chunks
    gain = gain_ref[0:1, :]
    rows = []
    for d in range(owners):
        scaled = [(x_ref[d, :, t, :].astype(F32) * gain).astype(BF16) for t in range(steps)]
        for c in range(chunks):
            rows += [x[c * each : (c + 1) * each] for x in scaled]
    x = jnp.concatenate(rows, 0)
    size = each * steps
    width = weight_ref.shape[1]
    block = min(width, 256)
    for first in range(0, width, block):
        lanes = slice(first, first + block)
        product = dot(x, weight_ref[:, lanes])
        for i, out in enumerate(outs):
            c, d = divmod(i, owners)
            start = (d * chunks + c) * size
            out[:, lanes] = product[start : start + size].astype(out.dtype)


def project(x, gain, weight, chunks):
    owners, seqs, steps, _ = x.shape
    width = weight.shape[1]
    outs = pl.pallas_call(
        functools.partial(project_kernel, chunks),
        out_shape=[
            jax.ShapeDtypeStruct((seqs * steps // chunks, width), F32 if d == 0 else BF16)
            for _ in range(chunks)
            for d in range(owners)
        ],
        in_specs=[whole()] * 3,
        out_specs=[whole()] * (owners * chunks),
        compiler_params=limit(12),
        cost_estimate=pl.CostEstimate(
            flops=2 * x.size * width, bytes_accessed=4 * x.size, transcendentals=0
        ),
        name="project",
    )(x, gain, weight)
    return [outs[c * owners : (c + 1) * owners] for c in range(chunks)]


def spread_heads(ref, value, offset, stride, seqs, heads, steps, size, t):
    for h in range(heads):
        tile, lane = divmod(h * size, 128)
        part = value[:, tile * 128 : (tile + 1) * 128]
        if lane:
            part = pltpu.roll(part, 128 - lane, 1)
        ref[pl.ds(offset + h * steps + t, seqs, stride=stride), :] = part


def put_rows(ref, start, count, value, stride=None):
    for m in range(ref.shape[0]):
        ref[m, pl.ds(start, count, stride=stride), :] = value[:, m * 128 : (m + 1) * 128]


def get_rows(ref, start, count, stride=None):
    return jnp.concatenate(
        [ref[m, pl.ds(start, count, stride=stride), :] for m in range(ref.shape[0])], 1
    )


def own_heads(product, masks, group, steps):
    tile = group * steps
    total = None
    for m, mask in enumerate(masks):
        part = jnp.where(mask, product[m * tile : (m + 1) * tile], 0.0)
        total = part if total is None else total + part
    shift = steps
    acc = total
    for _ in range(group - 1):
        acc = acc + pltpu.roll(total, shift, 0)
        shift += steps
    return acc


def early_kernel(steps, size, axes, count, *refs):
    inputs = 12 + count
    sources, refs = refs[:inputs], refs[inputs:]
    outputs = 5 if count else 4
    outs, refs = refs[:outputs], refs[outputs:]
    out_ref, low_ref, stat_ref, const_ref = outs[:4]
    held, (kscr, pscr, uscr, gscr, sems) = refs[:12], refs[12:]
    k_ref, v_ref, b_ref, d_ref, a_ref, s0_ref = held[:6]
    tok_ref, gain_ref, beta_ref, decay_ref, base_ref, last_ref = held[6:]
    seqs, _, width = s0_ref.shape
    local = tok_ref.shape[2]
    part = block_of(axes[-1], local)
    views = list(sources[:7]) + [ref.at[:, part] for ref in sources[7:10]] + list(sources[10:12])
    copies = fetch(views, held, sems)
    if count:
        wide = sources[12].shape[1]
        targets = [outs[4].at[:, i * wide : (i + 1) * wide] for i in range(count)]
        copies += fetch(sources[12:], targets, sems.at[pl.ds(12, count)])
    for copy in copies[:5]:
        copy.wait()
    heads = width // size
    group = 8 // steps
    ones = head_ones(width, size)
    masks = [head_mask(g * group, group, steps, width, size) for g in range(heads // group)]
    pick = jnp.where(
        lax.broadcasted_iota(jnp.int32, (heads, width), 0)
        == lax.broadcasted_iota(jnp.int32, (heads, width), 1) // size,
        1.0,
        0.0,
    )
    keys = [k_ref[:, t, :].astype(F32) for t in range(steps)]
    for t in range(steps):
        spread_heads(kscr, keys[t], 0, heads * steps, seqs, heads, steps, size, t)
    pairs = [(t, r) for t in range(steps) for r in range(t + 1)]
    sums = head_sum(jnp.concatenate([keys[t] * keys[r] for t, r in pairs], 0), ones)
    raw = {p: sums[i * seqs : (i + 1) * seqs] for i, p in enumerate(pairs)}
    inv = [lax.rsqrt(raw[t, t] + EPS) for t in range(steps)]

    copies[5].wait()

    def read(s, carry):
        kb = kscr[pl.ds(s * heads * steps, heads * steps), :][:, :size].astype(BF16)
        seen = own_heads(dot(kb, s0_ref[s].astype(BF16)), masks, group, steps)
        put_rows(pscr, s * 8, 8, seen)
        return carry

    lax.fori_loop(0, seqs, read, 0, unroll=8)
    highest = lax.Precision.HIGHEST
    cumul, solved = [], []
    for t in range(steps):
        live = jnp.where(a_ref[...] > t, 1.0, 0.0)
        log = dot(d_ref[t] * live, pick, ((0,), (0,)), highest)
        strength = dot(jax.nn.sigmoid(b_ref[t]) * live, pick, ((0,), (0,)), highest)
        cumul.append(log if t == 0 else cumul[-1] + log)
        seen = get_rows(pscr, t, seqs, 8) * inv[t]
        rest = v_ref[:, t, :].astype(F32) - jnp.exp(cumul[t]) * seen
        for r in range(t):
            rest = rest - jnp.exp(cumul[t] - cumul[r]) * (raw[t, r] * inv[t] * inv[r]) * solved[r]
        solved.append(strength * rest)
    for t in range(steps):
        add = jnp.exp(cumul[-1] - cumul[t]) * inv[t] * solved[t]
        for g in range(group):
            put_rows(uscr, g * steps + t, seqs, add, 8)
    gscr[...] = jnp.exp(cumul[-1])

    def write(s, carry):
        ub = get_rows(uscr, s * 8, 8)
        wide = jnp.concatenate([jnp.where(m, ub, 0.0) for m in masks], 0).astype(BF16)
        kb = kscr[pl.ds(s * heads * steps, heads * steps), :][:, :size].astype(BF16)
        new = gscr[pl.ds(s, 1), :] * s0_ref[s] + dot(kb, wide, ((0,), (0,)))
        out_ref[s] = new
        low_ref[s] = new.astype(BF16)
        return carry

    lax.fori_loop(0, seqs, write, 0, unroll=8)
    for copy in copies[6:]:
        copy.wait()
    statistics(steps, tok_ref, gain_ref, beta_ref, decay_ref, stat_ref)
    entry = jnp.where(
        lax.broadcasted_iota(jnp.int32, (size, width), 0)
        == lax.broadcasted_iota(jnp.int32, (size, width), 1) % size,
        1.0,
        0.0,
    )
    const_ref[0:1, :] = dot(base_ref[...], pick, precision=highest)
    const_ref[1:2, :] = dot(last_ref[...], entry, precision=highest)


def early(axes, state, prev, tokens, in_gain, w_beta, w_decay, decay_base, out_gain, weights):
    prev_keys, prev_values, prev_beta, prev_decay, accepted = prev
    seqs, size, width = state.shape
    _, steps, local = tokens.shape
    heads = width // size
    heads_all = w_beta.shape[1]
    arrays = (
        prev_keys,
        prev_values,
        jnp.transpose(prev_beta, (1, 2, 0)),
        jnp.transpose(prev_decay, (1, 2, 0)),
        accepted.reshape(1, -1),
        state,
        tokens,
        in_gain.reshape(1, -1),
        w_beta.T,
        w_decay.T,
        decay_base.reshape(1, -1),
        out_gain.reshape(1, -1),
    )
    held = [like(a) for a in arrays]
    held[7] = VMEM((1, local), F32)
    held[8] = held[9] = VMEM((heads_all, local), BF16)
    shapes = [
        jax.ShapeDtypeStruct(state.shape, F32),
        jax.ShapeDtypeStruct(state.shape, BF16),
        jax.ShapeDtypeStruct((2 * heads_all + 8, seqs * steps), F32),
        jax.ShapeDtypeStruct((8, width), F32),
    ]
    if weights:
        rows, columns = weights[0].shape
        shapes.append(jax.ShapeDtypeStruct((rows, columns * len(weights)), BF16))
    return pl.pallas_call(
        functools.partial(early_kernel, steps, size, axes, len(weights)),
        out_shape=shapes,
        in_specs=[whole(HBM)] * (12 + len(weights)),
        out_specs=[whole()] * len(shapes),
        scratch_shapes=held
        + [
            VMEM((seqs * heads * steps, 128), F32),
            VMEM((width // 128, seqs * 8, 128), F32),
            VMEM((width // 128, seqs * 8, 128), F32),
            VMEM((seqs, width), F32),
            pltpu.SemaphoreType.DMA((12 + len(weights),)),
        ],
        cost_estimate=pl.CostEstimate(
            flops=seqs * 4000000, bytes_accessed=8 * state.size, transcendentals=0
        ),
        compiler_params=limit(20),
        name="early",
    )(*[pltpu.with_memory_space_constraint(a, HBM) for a in arrays + tuple(weights)])


def propose_kernel(dims, axes, parts, sources, blocks, first, stat_ref, const_ref, s_ref, *refs):
    steps, size, features, heads_all = dims
    part_refs, refs = refs[:parts], refs[parts:]
    block_refs, refs = refs[:sources], refs[sources:]
    out_refs, (kscr, pscr, wo, sems) = refs[:-4], refs[-4:]
    seqs = part_refs[0].shape[0] // steps
    width = s_ref.shape[2]
    heads = width // size
    group = 8 // steps
    place = [lax.axis_index(axis) for axis in axes]
    tp = place[-1]

    targets = [wo.at[lax.bitwise_xor(place[1], mark)] for mark in blocks]
    copies = fetch(block_refs, targets, sems)

    ones = head_ones(width, size)
    masks = [head_mask(g * group, group, steps, width, size) for g in range(heads // group)]
    rows = seqs * steps
    stat = stat_ref[...]
    count = stat.shape[0]
    src = lax.broadcasted_iota(jnp.int32, (count, width), 0)
    head = lax.broadcasted_iota(jnp.int32, (count, width), 1) // size + tp * heads
    highest = lax.Precision.HIGHEST
    flat = stat.T
    base, gain = const_ref[0:1, :], const_ref[1:2, :]

    def take(row):
        return dot(flat, jnp.where(src == row, 1.0, 0.0), precision=highest)

    scale = lax.rsqrt(take(2 * heads_all) / features + EPS)
    strength = jax.nn.sigmoid(scale * take(head))
    rate = scale * take(heads_all + head)
    log = -base * (jnp.maximum(rate, 0.0) + jnp.log1p(jnp.exp(-jnp.abs(rate))))

    def column(w):
        lanes = slice(w * width, (w + 1) * width)
        total = part_refs[0][:, lanes].astype(F32)
        for ref in part_refs[1:]:
            total = total + ref[:, lanes].astype(F32)
        return total * scale

    query, key = column(0), column(1)
    squares = head_sum(jnp.concatenate([query * query, key * key], 0), ones)
    query = query * (lax.rsqrt(squares[:rows] + EPS) * size ** (-0.5))
    key = key * lax.rsqrt(squares[rows:] + EPS)

    def at(array, t):
        return array[t * seqs : (t + 1) * seqs]

    stride = 2 * heads * steps
    for t in range(steps):
        spread_heads(kscr, at(query, t), 0, stride, seqs, heads, steps, size, t)
        spread_heads(kscr, at(key, t), heads * steps, stride, seqs, heads, steps, size, t)
    below = [(t, r) for t in range(steps) for r in range(t)]
    inside = [(t, r) for t in range(steps) for r in range(t + 1)]
    products = [at(key, t) * at(key, r) for t, r in below]
    products += [at(query, t) * at(key, r) for t, r in inside]
    sums = head_sum(jnp.concatenate(products, 0), ones)
    k_k = {p: at(sums, i) for i, p in enumerate(below)}
    q_k = {p: at(sums, len(below) + i) for i, p in enumerate(inside)}
    upper = lax.broadcasted_iota(jnp.int32, (8, width), 0) < steps

    def read(s, carry):
        vectors = kscr[pl.ds(s * stride, stride), :][:, :size].astype(BF16)
        seen = dot(vectors, s_ref[first * seqs + s])
        half = heads * steps
        from_query = own_heads(seen[:half], masks, group, steps)
        from_key = own_heads(seen[half:], masks, group, steps)
        put_rows(pscr, s * 8, 8, jnp.where(upper, from_query, from_key))
        return carry

    lax.fori_loop(0, seqs, read, 0, unroll=8)
    value, gate = column(2), column(3)
    cumul, solved, outs = [], [], []
    for t in range(steps):
        cumul.append(at(log, t) if t == 0 else cumul[-1] + at(log, t))
        grown = jnp.exp(cumul[t])
        rest = at(value, t) - grown * get_rows(pscr, steps + t, seqs, 8)
        out = grown * get_rows(pscr, t, seqs, 8)
        for r in range(t):
            decay = jnp.exp(cumul[t] - cumul[r])
            rest = rest - decay * k_k[t, r] * solved[r]
            out = out + decay * q_k[t, r] * solved[r]
        solved.append(at(strength, t) * rest)
        outs.append(out + q_k[t, t] * solved[t])
    output = jnp.concatenate(outs, 0)
    mean = head_sum(output * output, ones) * (1.0 / size)
    gated = output * lax.rsqrt(mean + EPS) * gain * (gate / (1.0 + jnp.exp(-gate)))
    gated = gated.astype(BF16)
    if not blocks:
        out_refs[0][...] = gated
        return
    for copy in copies:
        copy.wait()
    n = wo.shape[0]
    for s in list(range(1, n)) + [0]:
        out_refs[s][...] = dot(gated, wo[lax.rem(tp + s, n)]).astype(out_refs[s].dtype)


def propose(axes, stat, consts, state, parts, blocks, block_arrays, n_tp, dims, seqs, first):
    steps, size = dims[0], dims[1]
    width = state.shape[2]
    heads = width // size
    rows = seqs * steps
    if blocks:
        share = dims[2] // n_tp
        shapes = [
            jax.ShapeDtypeStruct((rows, share), F32 if s == 0 else BF16) for s in range(n_tp)
        ]
        wo = VMEM((n_tp, width, share), BF16)
    else:
        shapes = [jax.ShapeDtypeStruct((rows, width), BF16)]
        wo = VMEM((8, 128), F32)
    return pl.pallas_call(
        functools.partial(
            propose_kernel, dims, axes, len(parts), len(block_arrays), blocks, first
        ),
        out_shape=shapes,
        in_specs=[whole()] * (3 + len(parts)) + [whole(HBM)] * len(block_arrays),
        out_specs=[whole()] * len(shapes),
        scratch_shapes=[
            VMEM((seqs * 2 * heads * steps, 128), F32),
            VMEM((width // 128, seqs * 8, 128), F32),
            wo,
            pltpu.SemaphoreType.DMA((max(1, len(blocks)),)),
        ],
        compiler_params=limit(24),
        cost_estimate=pl.CostEstimate(
            flops=seqs * 4000000, bytes_accessed=4 * state.size, transcendentals=0
        ),
        name="propose",
    )(stat, consts, state, *parts, *block_arrays)


def finish_kernel(steps, chunks, *refs):
    ins, out_ref = refs[:-1], refs[-1]
    per = len(ins) // chunks
    each = out_ref.shape[0] // chunks
    for c in range(chunks):
        total = ins[c * per][...].astype(F32)
        for ref in ins[c * per + 1 : (c + 1) * per]:
            total = total + ref[...].astype(F32)
        for t in range(steps):
            out_ref[c * each : (c + 1) * each, t, :] = total[t * each : (t + 1) * each].astype(
                out_ref.dtype
            )


def finish(pieces, seqs, steps):
    chunks = len(pieces)
    flat = [a for piece in pieces for a in piece]
    return pl.pallas_call(
        functools.partial(finish_kernel, steps, chunks),
        out_shape=jax.ShapeDtypeStruct((seqs, steps, flat[0].shape[1]), BF16),
        in_specs=[whole()] * len(flat),
        out_specs=whole(),
        compiler_params=limit(8),
        name="finish",
    )(*flat)


def body(sizes, *args):
    return layer(sizes, *args)


def layer(
    sizes,
    tokens,
    in_gain,
    w_query,
    w_key,
    w_value,
    w_gate,
    w_beta,
    w_decay,
    decay_base,
    out_gain,
    w_out,
    state,
    prev_keys,
    prev_values,
    prev_beta,
    prev_decay,
    accepted,
):
    n_grp, n_kv, n_tp = sizes
    seqs, steps, local = tokens.shape
    size = out_gain.shape[0]
    features = in_gain.shape[0]
    heads_all = w_beta.shape[1]
    dims = (steps, size, features, heads_all)
    square = n_kv == n_tp and n_kv & (n_kv - 1) == 0 and n_grp == 2
    chunks = CHUNKS if square else 1
    each = seqs // chunks
    axes = ("grp", "kv", "tp")
    weights = (w_query, w_key, w_value, w_gate)
    prev = (prev_keys, prev_values, prev_beta, prev_decay, accepted)

    def ring(n, s):
        return [(i, (i + s) % n) for i in range(n)]

    if square:
        n = n_kv
        turn = [(k * n + t, t * n + (k - t) % n) for k in range(n) for t in range(n)]
        turned = lax.ppermute(tokens, ("kv", "tp"), turn)
    new_state, low, stat, consts, *staged = early(
        axes, state, prev, tokens, in_gain, w_beta, w_decay, decay_base, out_gain,
        weights if square else (),
    )
    if square:
        own_rows = lax.dynamic_slice_in_dim(
            in_gain.reshape(1, -1), lax.axis_index("kv") * local, local, 1
        )
        own_rows = jnp.broadcast_to(own_rows, (8, local))
        staged, later = lax.optimization_barrier((staged, w_out))
        turned, staged = lax.optimization_barrier((turned, staged))
        arrays, marks = [w_out], [0]
        bits = [n >> i for i in range(1, n.bit_length())]

        def swap(array, bit):
            return lax.ppermute(array, "kv", [(i, i ^ bit) for i in range(n)])

        for bit in bits:
            arrays.append(swap(later, bit))
            marks.append(bit)
        gathered = lax.all_gather(turned, "tp")
        parts = project(gathered, own_rows, staged[0], chunks)
        parts = [
            [piece[0]] + [lax.ppermute(piece[d], "kv", ring(n, d)) for d in range(1, n)]
            for piece in parts
        ]
        stat, arrays, parts[0][0] = lax.optimization_barrier((stat, arrays, parts[0][0]))
        for i, bit in enumerate(bits[1:], 1):
            for j in range(len(arrays)):
                mark = marks[j] ^ bit
                if mark not in marks:
                    arrays.append(swap(arrays[j], bit))
                    marks.append(mark)
    else:
        arrays, marks = [], []
        x = lax.all_gather(tokens, "tp", axis=2, tiled=True)
        x = jnp.transpose(x, (1, 0, 2)).reshape(seqs * steps, -1)
        x = (x.astype(F32) * in_gain).astype(BF16)
        full = [lax.all_gather(w, "kv", axis=0, tiled=True) for w in weights]
        products = [jnp.dot(x, w, preferred_element_type=F32) for w in full]
        parts = [[jnp.concatenate(products, 1)]]

    stat_all = jnp.sum(lax.all_gather(stat, "tp"), 0)
    by_step = stat_all.reshape(stat_all.shape[0], steps, seqs)
    pieces = []
    for c in range(chunks):
        own = by_step[:, :, c * each : (c + 1) * each].reshape(stat_all.shape[0], -1)
        out = propose(
            axes, own, consts, low, parts[c], marks, arrays, n_tp, dims, each, c
        )
        if square:
            pieces.append(
                [out[0]] + [lax.ppermute(out[s], "tp", ring(n_tp, s)) for s in range(1, n_tp)]
            )
        else:
            full = lax.all_gather(w_out, "kv", axis=1, tiled=True)
            terms = jnp.dot(out[0], full, preferred_element_type=F32).astype(BF16)
            pieces.append([lax.psum_scatter(terms, "tp", scatter_dimension=1, tiled=True)])
    return finish(pieces, seqs, steps), new_state


def solution(mesh):
    rows = P(("grp", "kv"), None, "tp")
    matrix = P("kv", "tp")
    placed = (
        rows,
        P(),
        matrix,
        matrix,
        matrix,
        matrix,
        P(),
        P(),
        P("tp"),
        P(),
        P("tp", "kv"),
        rows,
        rows,
        rows,
        rows,
        rows,
        P(("grp", "kv")),
    )
    sizes = (mesh.shape["grp"], mesh.shape["kv"], mesh.shape["tp"])
    return jax.shard_map(
        functools.partial(body, sizes),
        mesh=mesh,
        in_specs=placed,
        out_specs=(rows, rows),
        check_vma=False,
    )
```

```python
import functools

import jax
import jax.numpy as jnp
from jax import lax
from jax.experimental import pallas as pl
from jax.experimental.pallas import tpu as pltpu
from jax.sharding import PartitionSpec as P

EPS = 1e-06
F32 = jnp.float32
BF16 = jnp.bfloat16
VMEM = pltpu.VMEM
HBM = pltpu.HBM


def whole(space=VMEM):
    return pl.BlockSpec(memory_space=space)


def fetch(sources, targets, sems):
    copies = [
        pltpu.make_async_copy(source, target, sems.at[i])
        for i, (source, target) in enumerate(zip(sources, targets))
    ]
    for copy in copies:
        copy.start()
    return copies


def like(array):
    return VMEM(array.shape, array.dtype)


def limit(mebibytes):
    return pltpu.CompilerParams(vmem_limit_bytes=mebibytes << 20)


def dot(a, b, contract=((1,), (0,)), precision=None):
    return lax.dot_general(
        a, b, (contract, ((), ())), precision=precision, preferred_element_type=F32
    )


def head_ones(width, size):
    row = lax.broadcasted_iota(jnp.int32, (width, width), 0) // size
    col = lax.broadcasted_iota(jnp.int32, (width, width), 1) // size
    return jnp.where(row == col, 1.0, 0.0).astype(BF16)


def head_sum(values, ones):
    high = values.astype(BF16)
    low = (values - high.astype(F32)).astype(BF16)
    return dot(high, ones) + dot(low, ones)


def head_mask(first, group, steps, width, size):
    sub = lax.broadcasted_iota(jnp.int32, (group * steps, width), 0) // steps + first
    lane = lax.broadcasted_iota(jnp.int32, (group * steps, width), 1) // size
    return sub == lane


def block_of(axis, size):
    return pl.ds(pl.multiple_of(lax.axis_index(axis) * size, size), size)


def stat_rows(values):
    high = values.astype(BF16).astype(F32)
    return high, values - high


def project_kernel(chunks, x_ref, gain_ref, weight_ref, small_ref, *outs):
    owners, _, steps, local = x_ref.shape
    gain = gain_ref[0:1, :]
    raw, spans, start = [], [], 0
    tokens = [[x_ref[d, :, t, :].astype(F32) for t in range(steps)] for d in range(owners)]
    for first, each in chunks:
        for d in range(owners):
            raw += [x[first : first + each] for x in tokens[d]]
            spans.append(slice(start, start + each * steps))
            start += each * steps
    raw = jnp.concatenate(raw, 0)
    x = (raw * gain).astype(BF16)
    square = raw * raw
    high = square.astype(BF16)
    low = (square - high.astype(F32)).astype(BF16)
    count = small_ref.shape[0]
    unit = (lax.broadcasted_iota(jnp.int32, (128, local), 0) == count).astype(F32).astype(BF16)
    small = jnp.concatenate([small_ref[...], jnp.zeros((128 - count, local), BF16)], 0)
    sums = dot(x, small, ((1,), (1,))) + dot(high, unit, ((1,), (1,))) + dot(low, unit, ((1,), (1,)))
    for out, span in zip(outs, spans):
        rows = span.stop - span.start
        part = sums[span]
        if rows < 128:
            part = jnp.concatenate([part, jnp.zeros((128 - rows, 128), F32)], 0)
        part = part.T
        extra = []
        for first in range(0, 2 * count, count):
            extra += stat_rows(part[first : first + count])
        extra.append(jnp.zeros((count, out.shape[1] - 128 * len(extra)), F32))
        out[rows : rows + count, :] = jnp.concatenate(extra, 1).astype(out.dtype)
    width = weight_ref.shape[1]
    block = min(width, 256)
    for first in range(0, width, block):
        lanes = slice(first, first + block)
        product = dot(x, weight_ref[:, lanes])
        for out, span in zip(outs, spans):
            rows = span.stop - span.start
            out[:rows, lanes] = product[span].astype(out.dtype)


def project(x, gain, weight, small, chunks):
    owners, _, steps, _ = x.shape
    width = weight.shape[1]
    extra = small.shape[0]
    outs = pl.pallas_call(
        functools.partial(project_kernel, chunks),
        out_shape=[
            jax.ShapeDtypeStruct((each * steps + extra, width), F32 if d == 0 else BF16)
            for _, each in chunks
            for d in range(owners)
        ],
        in_specs=[whole()] * 4,
        out_specs=[whole()] * (owners * len(chunks)),
        compiler_params=limit(16),
        cost_estimate=pl.CostEstimate(
            flops=2 * x.size * width, bytes_accessed=4 * x.size, transcendentals=0
        ),
        name="project",
    )(x, gain, weight, small)
    return [list(outs[c * owners : (c + 1) * owners]) for c in range(len(chunks))]


def assemble_kernel(axes, blocks, *refs):
    sources, out_ref, sems = refs[:-2], refs[-2], refs[-1]
    place = [lax.axis_index(axis) for axis in axes]
    targets = []
    for ref, (mark, flip) in zip(sources, blocks):
        target = out_ref.at[lax.bitwise_xor(place[1], mark)]
        if flip is not None:
            count = ref.shape[0]
            row = lax.bitwise_xor(place[0], flip) * count
            target = target.at[pl.ds(pl.multiple_of(row, count), count)]
        targets.append(target)
    for copy in fetch(sources, targets, sems):
        copy.wait()


def assemble(axes, arrays, blocks, n):
    return pl.pallas_call(
        functools.partial(assemble_kernel, axes, blocks),
        out_shape=jax.ShapeDtypeStruct((n,) + arrays[0].shape, arrays[0].dtype),
        in_specs=[whole(HBM)] * len(arrays),
        out_specs=whole(),
        scratch_shapes=[pltpu.SemaphoreType.DMA((len(arrays),))],
        compiler_params=limit(4),
        cost_estimate=pl.CostEstimate(
            flops=4000000, bytes_accessed=8 * arrays[0].size, transcendentals=0
        ),
        name="assemble",
    )(*arrays)


def spread_heads(ref, value, offset, stride, seqs, heads, steps, size, t):
    for h in range(heads):
        tile, lane = divmod(h * size, 128)
        part = value[:, tile * 128 : (tile + 1) * 128]
        if lane:
            part = pltpu.roll(part, 128 - lane, 1)
        ref[pl.ds(offset + h * steps + t, seqs, stride=stride), :] = part


def put_rows(ref, start, count, value, stride=None):
    for m in range(ref.shape[0]):
        ref[m, pl.ds(start, count, stride=stride), :] = value[:, m * 128 : (m + 1) * 128]


def get_rows(ref, start, count, stride=None):
    return jnp.concatenate(
        [ref[m, pl.ds(start, count, stride=stride), :] for m in range(ref.shape[0])], 1
    )


def own_heads(product, masks, group, steps):
    tile = group * steps
    total = None
    for m, mask in enumerate(masks):
        part = jnp.where(mask, product[m * tile : (m + 1) * tile], 0.0)
        total = part if total is None else total + part
    shift = steps
    acc = total
    for _ in range(group - 1):
        acc = acc + pltpu.roll(total, shift, 0)
        shift += steps
    return acc


def early_kernel(steps, size, axes, count, *refs):
    inputs = 12 + count if count else 8
    own = 11 if count else 8
    sources, refs = refs[:inputs], refs[inputs:]
    outputs = 7 if count else 3
    outs, refs = refs[:outputs], refs[outputs:]
    out_ref, low_ref, const_ref = outs[:3]
    held, (kscr, pscr, uscr, gscr, sems) = refs[:own], refs[own:]
    k_ref, v_ref, b_ref, d_ref, a_ref, s0_ref = held[:6]
    base_ref, last_ref = held[6:8]
    seqs, _, width = s0_ref.shape
    views = list(sources[:8])
    if count:
        part = block_of(axes[1], held[8].shape[1])
        views += [ref.at[:, part] for ref in sources[8:11]]
    copies = fetch(views, held, sems)
    if count:
        half = sources[-1].at[block_of(axes[0], outs[6].shape[0])]
        wide = sources[11].shape[1]
        targets = [outs[3].at[:, i * wide : (i + 1) * wide] for i in range(count)]
        copies += fetch(
            [half] + list(sources[11:-1]), [outs[6]] + targets, sems.at[pl.ds(11, count + 1)]
        )
    for copy in copies[:5]:
        copy.wait()
    heads = width // size
    group = 8 // steps
    ones = head_ones(width, size)
    masks = [head_mask(g * group, group, steps, width, size) for g in range(heads // group)]
    pick = jnp.where(
        lax.broadcasted_iota(jnp.int32, (heads, width), 0)
        == lax.broadcasted_iota(jnp.int32, (heads, width), 1) // size,
        1.0,
        0.0,
    )
    keys = [k_ref[:, t, :].astype(F32) for t in range(steps)]
    for t in range(steps):
        spread_heads(kscr, keys[t], 0, heads * steps, seqs, heads, steps, size, t)
    pairs = [(t, r) for t in range(steps) for r in range(t + 1)]
    sums = head_sum(jnp.concatenate([keys[t] * keys[r] for t, r in pairs], 0), ones)
    raw = {p: sums[i * seqs : (i + 1) * seqs] for i, p in enumerate(pairs)}
    inv = [lax.rsqrt(raw[t, t] + EPS) for t in range(steps)]

    copies[5].wait()

    def read(s, carry):
        kb = kscr[pl.ds(s * heads * steps, heads * steps), :][:, :size].astype(BF16)
        seen = own_heads(dot(kb, s0_ref[s].astype(BF16)), masks, group, steps)
        put_rows(pscr, s * 8, 8, seen)
        return carry

    lax.fori_loop(0, seqs, read, 0, unroll=8)
    highest = lax.Precision.HIGHEST
    cumul, solved = [], []
    for t in range(steps):
        live = jnp.where(a_ref[...] > t, 1.0, 0.0)
        log = dot(d_ref[t] * live, pick, ((0,), (0,)), highest)
        strength = dot(jax.nn.sigmoid(b_ref[t]) * live, pick, ((0,), (0,)), highest)
        cumul.append(log if t == 0 else cumul[-1] + log)
        seen = get_rows(pscr, t, seqs, 8) * inv[t]
        rest = v_ref[:, t, :].astype(F32) - jnp.exp(cumul[t]) * seen
        for r in range(t):
            rest = rest - jnp.exp(cumul[t] - cumul[r]) * (raw[t, r] * inv[t] * inv[r]) * solved[r]
        solved.append(strength * rest)
    for t in range(steps):
        add = jnp.exp(cumul[-1] - cumul[t]) * inv[t] * solved[t]
        for g in range(group):
            put_rows(uscr, g * steps + t, seqs, add, 8)
    gscr[...] = jnp.exp(cumul[-1])

    def write(s, carry):
        ub = get_rows(uscr, s * 8, 8)
        wide = jnp.concatenate([jnp.where(m, ub, 0.0) for m in masks], 0).astype(BF16)
        kb = kscr[pl.ds(s * heads * steps, heads * steps), :][:, :size].astype(BF16)
        new = gscr[pl.ds(s, 1), :] * s0_ref[s] + dot(kb, wide, ((0,), (0,)))
        out_ref[s] = new
        low_ref[s] = new.astype(BF16)
        return carry

    lax.fori_loop(0, seqs, write, 0, unroll=8)
    for copy in copies[6:]:
        copy.wait()
    if count:
        outs[4][0:1, :] = held[8][...]
        total = None
        for i, ref in enumerate(held[9:11]):
            rows, every = outs[5].shape[0], ref.shape[0]
            row = lax.broadcasted_iota(jnp.int32, (rows, every), 0) - i * heads
            col = lax.broadcasted_iota(jnp.int32, (rows, every), 1)
            chosen = (row >= 0) & (row < heads) & (col == row + lax.axis_index(axes[2]) * heads)
            term = dot(chosen.astype(F32).astype(BF16), ref[...])
            total = term if total is None else total + term
        outs[5][...] = total.astype(BF16)
    entry = jnp.where(
        lax.broadcasted_iota(jnp.int32, (size, width), 0)
        == lax.broadcasted_iota(jnp.int32, (size, width), 1) % size,
        1.0,
        0.0,
    )
    const_ref[0:1, :] = dot(base_ref[...], pick, precision=highest)
    const_ref[1:2, :] = dot(last_ref[...], entry, precision=highest)


def early(axes, state, prev, decay_base, out_gain, shared):
    prev_keys, prev_values, prev_beta, prev_decay, accepted = prev
    seqs, size, width = state.shape
    steps = prev_keys.shape[1]
    heads = width // size
    arrays = (
        prev_keys,
        prev_values,
        jnp.transpose(prev_beta, (1, 2, 0)),
        jnp.transpose(prev_decay, (1, 2, 0)),
        accepted.reshape(1, -1),
        state,
        decay_base.reshape(1, -1),
        out_gain.reshape(1, -1),
    )
    held = [like(a) for a in arrays]
    shapes = [
        jax.ShapeDtypeStruct(state.shape, F32),
        jax.ShapeDtypeStruct(state.shape, BF16),
        jax.ShapeDtypeStruct((8, width), F32),
    ]
    count = 0
    if shared:
        in_gain, w_beta, w_decay, weights, w_out = shared
        count = len(weights)
        rows, columns = weights[0].shape
        arrays += (in_gain.reshape(1, -1), w_beta.T, w_decay.T) + weights + (w_out,)
        small = VMEM((w_beta.shape[1], rows), BF16)
        held += [VMEM((1, rows), F32), small, small]
        shapes += [
            jax.ShapeDtypeStruct((rows, columns * count), BF16),
            jax.ShapeDtypeStruct((8, rows), F32),
            jax.ShapeDtypeStruct((-(-2 * heads // 8) * 8, rows), BF16),
            jax.ShapeDtypeStruct((w_out.shape[0] // 2, w_out.shape[1]), BF16),
        ]
    return pl.pallas_call(
        functools.partial(early_kernel, steps, size, axes, count),
        out_shape=shapes,
        in_specs=[whole(HBM)] * len(arrays),
        out_specs=[whole()] * len(shapes),
        scratch_shapes=held
        + [
            VMEM((seqs * heads * steps, 128), F32),
            VMEM((width // 128, seqs * 8, 128), F32),
            VMEM((width // 128, seqs * 8, 128), F32),
            VMEM((seqs, width), F32),
            pltpu.SemaphoreType.DMA((len(arrays),)),
        ],
        cost_estimate=pl.CostEstimate(
            flops=seqs * 4000000, bytes_accessed=8 * state.size, transcendentals=0
        ),
        compiler_params=limit(20),
        name="early",
    )(*[pltpu.with_memory_space_constraint(a, HBM) for a in arrays])


def propose_kernel(dims, axis, parts, first, const_ref, s_ref, *refs):
    steps, size, features = dims
    part_refs, wo, refs = refs[:parts], refs[parts], refs[parts + 1 :]
    out_refs, (kscr, pscr) = refs[:-2], refs[-2:]
    width = s_ref.shape[2]
    extra = -(-2 * (width // size) // 8) * 8
    seqs = (part_refs[0].shape[0] - extra) // steps
    heads = width // size
    group = 8 // steps
    ones = head_ones(width, size)
    masks = [head_mask(g * group, group, steps, width, size) for g in range(heads // group)]
    rows = seqs * steps

    def gathered(rows_of, lanes):
        total = part_refs[0][rows_of, lanes].astype(F32)
        for ref in part_refs[1:]:
            total = total + ref[rows_of, lanes].astype(F32)
        return total

    stat = gathered(slice(rows, rows + extra), slice(0, 512))
    logits = stat[:, :128] + stat[:, 128:256]
    total = stat[:, 256:384] + stat[:, 384:]
    flat = jnp.concatenate([logits, total], 0).T[:rows]
    src = lax.broadcasted_iota(jnp.int32, (2 * extra, width), 0)
    head = lax.broadcasted_iota(jnp.int32, (2 * extra, width), 1) // size
    highest = lax.Precision.HIGHEST
    base, gain = const_ref[0:1, :], const_ref[1:2, :]

    def take(row):
        return dot(flat, jnp.where(src == row, 1.0, 0.0), precision=highest)

    scale = lax.rsqrt(take(extra) / features + EPS)
    strength = jax.nn.sigmoid(scale * take(head))
    rate = scale * take(heads + head)
    log = -base * (jnp.maximum(rate, 0.0) + jnp.log1p(jnp.exp(-jnp.abs(rate))))

    def column(w):
        return gathered(slice(0, rows), slice(w * width, (w + 1) * width)) * scale

    query, key = column(0), column(1)
    squares = head_sum(jnp.concatenate([query * query, key * key], 0), ones)
    query = query * (lax.rsqrt(squares[:rows] + EPS) * size ** (-0.5))
    key = key * lax.rsqrt(squares[rows:] + EPS)

    def at(array, t):
        return array[t * seqs : (t + 1) * seqs]

    stride = 2 * heads * steps
    for t in range(steps):
        spread_heads(kscr, at(query, t), 0, stride, seqs, heads, steps, size, t)
        spread_heads(kscr, at(key, t), heads * steps, stride, seqs, heads, steps, size, t)
    below = [(t, r) for t in range(steps) for r in range(t)]
    inside = [(t, r) for t in range(steps) for r in range(t + 1)]
    products = [at(key, t) * at(key, r) for t, r in below]
    products += [at(query, t) * at(key, r) for t, r in inside]
    sums = head_sum(jnp.concatenate(products, 0), ones)
    k_k = {p: at(sums, i) for i, p in enumerate(below)}
    q_k = {p: at(sums, len(below) + i) for i, p in enumerate(inside)}
    upper = lax.broadcasted_iota(jnp.int32, (8, width), 0) < steps

    def read(s, carry):
        vectors = kscr[pl.ds(s * stride, stride), :][:, :size].astype(BF16)
        seen = dot(vectors, s_ref[first + s])
        half = heads * steps
        from_query = own_heads(seen[:half], masks, group, steps)
        from_key = own_heads(seen[half:], masks, group, steps)
        put_rows(pscr, s * 8, 8, jnp.where(upper, from_query, from_key))
        return carry

    lax.fori_loop(0, seqs, read, 0, unroll=8)
    value, gate = column(2), column(3)
    cumul, solved, outs = [], [], []
    for t in range(steps):
        cumul.append(at(log, t) if t == 0 else cumul[-1] + at(log, t))
        grown = jnp.exp(cumul[t])
        rest = at(value, t) - grown * get_rows(pscr, steps + t, seqs, 8)
        out = grown * get_rows(pscr, t, seqs, 8)
        for r in range(t):
            decay = jnp.exp(cumul[t] - cumul[r])
            rest = rest - decay * k_k[t, r] * solved[r]
            out = out + decay * q_k[t, r] * solved[r]
        solved.append(at(strength, t) * rest)
        outs.append(out + q_k[t, t] * solved[t])
    output = jnp.concatenate(outs, 0)
    mean = head_sum(output * output, ones) * (1.0 / size)
    gated = output * lax.rsqrt(mean + EPS) * gain * (gate / (1.0 + jnp.exp(-gate)))
    gated = gated.astype(BF16)
    n = wo.shape[0]
    tp = lax.axis_index(axis)
    for s in list(range(1, len(out_refs))) + [0]:
        block = wo[lax.rem(tp + s, n)] if n > 1 else wo[0]
        out_refs[s][...] = dot(gated, block).astype(out_refs[s].dtype)


def propose(axis, consts, state, parts, wo, dims, first, seqs):
    steps, size = dims[0], dims[1]
    width = state.shape[2]
    heads = width // size
    rows = seqs * steps
    shapes = [
        jax.ShapeDtypeStruct((rows, wo.shape[2]), F32 if s == 0 and wo.shape[0] > 1 else BF16)
        for s in range(wo.shape[0])
    ]
    return pl.pallas_call(
        functools.partial(propose_kernel, dims, axis, len(parts), first),
        out_shape=shapes,
        in_specs=[whole()] * (3 + len(parts)),
        out_specs=[whole()] * len(shapes),
        scratch_shapes=[
            VMEM((seqs * 2 * heads * steps, 128), F32),
            VMEM((width // 128, seqs * 8, 128), F32),
        ],
        compiler_params=limit(12),
        cost_estimate=pl.CostEstimate(
            flops=seqs * 4000000, bytes_accessed=4 * state.size, transcendentals=0
        ),
        name="propose",
    )(consts, state, *parts, wo)


def finish_kernel(steps, chunks, *refs):
    ins, out_ref = refs[:-1], refs[-1]
    per = len(ins) // len(chunks)
    for c, (first, each) in enumerate(chunks):
        total = ins[c * per][...].astype(F32)
        for ref in ins[c * per + 1 : (c + 1) * per]:
            total = total + ref[...].astype(F32)
        for t in range(steps):
            out_ref[first : first + each, t, :] = total[t * each : (t + 1) * each].astype(
                out_ref.dtype
            )


def finish(pieces, chunks, seqs, steps):
    flat = [a for piece in pieces for a in piece]
    return pl.pallas_call(
        functools.partial(finish_kernel, steps, chunks),
        out_shape=jax.ShapeDtypeStruct((seqs, steps, flat[0].shape[1]), BF16),
        in_specs=[whole()] * len(flat),
        out_specs=whole(),
        compiler_params=limit(8),
        name="finish",
    )(*flat)


def split(seqs):
    last = max(8, seqs // 4)
    return ((0, seqs - last), (seqs - last, last)) if seqs % 8 == 0 and seqs > 8 else ((0, seqs),)


def body(sizes, *args):
    return layer(sizes, *args)


def layer(
    sizes,
    tokens,
    in_gain,
    w_query,
    w_key,
    w_value,
    w_gate,
    w_beta,
    w_decay,
    decay_base,
    out_gain,
    w_out,
    state,
    prev_keys,
    prev_values,
    prev_beta,
    prev_decay,
    accepted,
):
    n_grp, n_kv, n_tp = sizes
    seqs, steps, _ = tokens.shape
    heads = decay_base.shape[0]
    size = out_gain.shape[0]
    features = in_gain.shape[0]
    dims = (steps, size, features)
    square = n_kv == n_tp and n_kv & (n_kv - 1) == 0 and n_grp == 2
    chunks = split(seqs) if square else ((0, seqs),)
    axes = ("grp", "kv", "tp")
    weights = (w_query, w_key, w_value, w_gate)
    prev = (prev_keys, prev_values, prev_beta, prev_decay, accepted)

    def ring(n, s):
        return [(i, (i + s) % n) for i in range(n)]

    if square:
        n = n_kv
        turn = [(k * n + t, t * n + (k - t) % n) for k in range(n) for t in range(n)]
        turned = lax.ppermute(tokens, ("kv", "tp"), turn)
    shared = (in_gain, w_beta, w_decay, weights, w_out) if square else None
    new_state, low, consts, *staged = early(axes, state, prev, decay_base, out_gain, shared)
    if square:
        weight, own_gain, small, mine = staged
        turned, weight = lax.optimization_barrier((turned, weight))
        halves, marks = [mine], [0]
        bits = [n >> i for i in range(1, n.bit_length())]

        def swap(array, bit):
            return lax.ppermute(array, "kv", [(i, i ^ bit) for i in range(n)])

        for bit in bits:
            halves.append(swap(mine, bit))
            marks.append(bit)
        gathered = lax.all_gather(turned, "tp")
        parts = project(gathered, own_gain, weight, small, chunks)
        for piece in parts:
            for d in range(1, n):
                piece[d] = lax.ppermute(piece[d], "kv", ring(n, d))
        halves, parts[0][0] = lax.optimization_barrier((halves, parts[0][0]))
        for bit in bits[1:]:
            for j in range(len(halves)):
                if marks[j] ^ bit not in marks:
                    halves.append(swap(halves[j], bit))
                    marks.append(marks[j] ^ bit)
        arrays, blocks = [w_out], [(0, None)]
        for i in range(1, len(halves)):
            other = lax.ppermute(halves[i], "grp", ring(n_grp, 1))
            arrays += [halves[i], other]
            blocks += [(marks[i], 0), (marks[i], 1)]
        wo = assemble(axes, arrays, blocks, n)
    else:
        x = lax.all_gather(tokens, "tp", axis=2, tiled=True)
        x = jnp.transpose(x, (1, 0, 2)).reshape(seqs * steps, -1).astype(F32)
        square_sum = jnp.sum(x * x, -1)
        x = (x * in_gain).astype(BF16)
        full = [lax.all_gather(w, "kv", axis=0, tiled=True) for w in weights]
        products = [jnp.dot(x, w, preferred_element_type=F32) for w in full]
        start = lax.axis_index("tp") * heads
        chosen = [lax.dynamic_slice_in_dim(w, start, heads, 1) for w in (w_beta, w_decay)]
        logits = jnp.dot(x, jnp.concatenate(chosen, 1), preferred_element_type=F32).T
        extra = -(-2 * heads // 8) * 8
        sums = jnp.zeros((extra, sum(p.shape[1] for p in products)), F32)
        sums = sums.at[: 2 * heads, : seqs * steps].set(logits)
        sums = sums.at[0, 256 : 256 + seqs * steps].set(square_sum)
        parts = [[jnp.concatenate([jnp.concatenate(products, 1), sums], 0)]]
        wo = lax.all_gather(w_out, "kv", axis=1, tiled=True)[None]

    pieces = []
    for (first, each), part in zip(chunks, parts):
        out = propose("tp", consts, low, part, wo, dims, first, each)
        if square:
            pieces.append(
                [out[0]] + [lax.ppermute(out[s], "tp", ring(n_tp, s)) for s in range(1, n_tp)]
            )
        else:
            pieces.append([lax.psum_scatter(out[0], "tp", scatter_dimension=1, tiled=True)])
    return finish(pieces, chunks, seqs, steps), new_state


def solution(mesh):
    rows = P(("grp", "kv"), None, "tp")
    matrix = P("kv", "tp")
    placed = (
        rows,
        P(),
        matrix,
        matrix,
        matrix,
        matrix,
        P(),
        P(),
        P("tp"),
        P(),
        P("tp", "kv"),
        rows,
        rows,
        rows,
        rows,
        rows,
        P(("grp", "kv")),
    )
    sizes = (mesh.shape["grp"], mesh.shape["kv"], mesh.shape["tp"])
    return jax.shard_map(
        functools.partial(body, sizes),
        mesh=mesh,
        in_specs=placed,
        out_specs=(rows, rows),
        check_vma=False,
    )
```

```python
import functools

import jax
import jax.numpy as jnp
from jax import lax
from jax.experimental import pallas as pl
from jax.experimental.pallas import tpu as pltpu
from jax.sharding import PartitionSpec as P

EPS = 1e-06
F32 = jnp.float32
BF16 = jnp.bfloat16
VMEM = pltpu.VMEM
HBM = pltpu.HBM


def whole(space=VMEM):
    return pl.BlockSpec(memory_space=space)


def fetch(sources, targets, sems):
    copies = [
        pltpu.make_async_copy(source, target, sems.at[i])
        for i, (source, target) in enumerate(zip(sources, targets))
    ]
    for copy in copies:
        copy.start()
    return copies


def like(array):
    return VMEM(array.shape, array.dtype)


def limit(mebibytes):
    return pltpu.CompilerParams(vmem_limit_bytes=mebibytes << 20)


def dot(a, b, contract=((1,), (0,)), precision=None):
    return lax.dot_general(
        a, b, (contract, ((), ())), precision=precision, preferred_element_type=F32
    )


def head_ones(width, size):
    row = lax.broadcasted_iota(jnp.int32, (width, width), 0) // size
    col = lax.broadcasted_iota(jnp.int32, (width, width), 1) // size
    return jnp.where(row == col, 1.0, 0.0).astype(BF16)


def head_sum(values, ones):
    high = values.astype(BF16)
    low = (values - high.astype(F32)).astype(BF16)
    return dot(high, ones) + dot(low, ones)


def head_mask(first, group, steps, width, size):
    sub = lax.broadcasted_iota(jnp.int32, (group * steps, width), 0) // steps + first
    lane = lax.broadcasted_iota(jnp.int32, (group * steps, width), 1) // size
    return sub == lane


def block_of(axis, size):
    return pl.ds(pl.multiple_of(lax.axis_index(axis) * size, size), size)


def stat_rows(values):
    high = values.astype(BF16).astype(F32)
    return high, values - high


def project_kernel(chunks, layout, x_ref, gain_ref, weight_ref, small_ref, *outs):
    owners, _, steps, local = x_ref.shape
    gain = gain_ref[0:1, :]
    raw, spans, start = [], {}, 0
    for d in range(owners):
        tokens = [x_ref[d, :, t, :].astype(F32) for t in range(steps)]
        for c, (first, each) in enumerate(chunks):
            raw += [x[first : first + each] for x in tokens]
            spans[d, c] = slice(start, start + each * steps)
            start += each * steps
    raw = jnp.concatenate(raw, 0)
    x = (raw * gain).astype(BF16)
    square = raw * raw
    high = square.astype(BF16)
    low = (square - high.astype(F32)).astype(BF16)
    count = small_ref.shape[0]
    unit = (lax.broadcasted_iota(jnp.int32, (128, local), 0) == count).astype(F32).astype(BF16)
    small = jnp.concatenate([small_ref[...], jnp.zeros((128 - count, local), BF16)], 0)
    sums = dot(x, small, ((1,), (1,))) + dot(high, unit, ((1,), (1,))) + dot(low, unit, ((1,), (1,)))
    width = weight_ref.shape[1]
    for out, (d, parts, with_sums) in zip(outs, layout):
        if not with_sums:
            continue
        extra = []
        for c in range(len(chunks)):
            part = sums[spans[d, c]]
            if part.shape[0] < 128:
                part = jnp.concatenate([part, jnp.zeros((128 - part.shape[0], 128), F32)], 0)
            part = part.T
            for first in range(0, 2 * count, count):
                extra += stat_rows(part[first : first + count])
        if width > 128 * len(extra):
            extra.append(jnp.zeros((count, width - 128 * len(extra)), F32))
        out[out.shape[0] - count :, :] = jnp.concatenate(extra, 1).astype(out.dtype)
    block = min(width, 256)
    for first in range(0, width, block):
        lanes = slice(first, first + block)
        product = dot(x, weight_ref[:, lanes])
        for out, (d, parts, _) in zip(outs, layout):
            start = 0
            for c in parts:
                piece = product[spans[d, c]]
                out[start : start + piece.shape[0], lanes] = piece.astype(out.dtype)
                start += piece.shape[0]


def project(x, gain, weight, small, chunks, layout):
    _, _, steps, _ = x.shape
    width = weight.shape[1]

    def shape(d, parts, with_sums, dtype):
        rows = sum(chunks[c][1] for c in parts) * steps
        return jax.ShapeDtypeStruct((rows + small.shape[0] * with_sums, width), dtype)

    return pl.pallas_call(
        functools.partial(project_kernel, chunks, [entry[:3] for entry in layout]),
        out_shape=[shape(*entry) for entry in layout],
        in_specs=[whole()] * 4,
        out_specs=[whole()] * len(layout),
        compiler_params=limit(16),
        cost_estimate=pl.CostEstimate(
            flops=2 * x.size * width, bytes_accessed=4 * x.size, transcendentals=0
        ),
    )(x, gain, weight, small)


def assemble_kernel(axes, blocks, *refs):
    sources, out_ref, sems = refs[:-2], refs[-2], refs[-1]
    place = [lax.axis_index(axis) for axis in axes]
    targets = []
    for ref, (mark, flip) in zip(sources, blocks):
        target = out_ref.at[lax.bitwise_xor(place[1], mark)]
        if flip is not None:
            count = ref.shape[0]
            row = lax.bitwise_xor(place[0], flip) * count
            target = target.at[pl.ds(pl.multiple_of(row, count), count)]
        targets.append(target)
    for copy in fetch(sources, targets, sems):
        copy.wait()


def assemble(axes, arrays, blocks, n):
    return pl.pallas_call(
        functools.partial(assemble_kernel, axes, blocks),
        out_shape=jax.ShapeDtypeStruct((n,) + arrays[0].shape, arrays[0].dtype),
        in_specs=[whole(HBM)] * len(arrays),
        out_specs=whole(),
        scratch_shapes=[pltpu.SemaphoreType.DMA((len(arrays),))],
        compiler_params=limit(4),
        cost_estimate=pl.CostEstimate(
            flops=4000000, bytes_accessed=8 * arrays[0].size, transcendentals=0
        ),
        name="assemble",
    )(*arrays)


def spread_heads(ref, value, offset, stride, seqs, heads, steps, size, t):
    for h in range(heads):
        tile, lane = divmod(h * size, 128)
        part = value[:, tile * 128 : (tile + 1) * 128]
        if lane:
            part = pltpu.roll(part, 128 - lane, 1)
        ref[pl.ds(offset + h * steps + t, seqs, stride=stride), :] = part


def put_rows(ref, start, count, value, stride=None):
    for m in range(ref.shape[0]):
        ref[m, pl.ds(start, count, stride=stride), :] = value[:, m * 128 : (m + 1) * 128]


def get_rows(ref, start, count, stride=None):
    return jnp.concatenate(
        [ref[m, pl.ds(start, count, stride=stride), :] for m in range(ref.shape[0])], 1
    )


def own_heads(product, masks, group, steps):
    tile = group * steps
    total = None
    for m, mask in enumerate(masks):
        part = jnp.where(mask, product[m * tile : (m + 1) * tile], 0.0)
        total = part if total is None else total + part
    shift = steps
    acc = total
    for _ in range(group - 1):
        acc = acc + pltpu.roll(total, shift, 0)
        shift += steps
    return acc


def early_kernel(steps, size, axes, count, *refs):
    inputs = 12 + count if count else 8
    own = 11 if count else 8
    sources, refs = refs[:inputs], refs[inputs:]
    outputs = 7 if count else 3
    outs, refs = refs[:outputs], refs[outputs:]
    out_ref, low_ref, const_ref = outs[:3]
    held, (kscr, pscr, uscr, gscr, sems) = refs[:own], refs[own:]
    k_ref, v_ref, b_ref, d_ref, a_ref, s0_ref = held[:6]
    base_ref, last_ref = held[6:8]
    seqs, _, width = s0_ref.shape
    views = list(sources[:8])
    if count:
        part = block_of(axes[1], held[8].shape[1])
        views += [ref.at[:, part] for ref in sources[8:11]]
    copies = fetch(views, held, sems)
    if count:
        half = sources[-1].at[block_of(axes[0], outs[6].shape[0])]
        wide = sources[11].shape[1]
        targets = [outs[3].at[:, i * wide : (i + 1) * wide] for i in range(count)]
        copies += fetch(
            [half] + list(sources[11:-1]), [outs[6]] + targets, sems.at[pl.ds(11, count + 1)]
        )
    for copy in copies[:5]:
        copy.wait()
    heads = width // size
    group = 8 // steps
    ones = head_ones(width, size)
    masks = [head_mask(g * group, group, steps, width, size) for g in range(heads // group)]
    pick = jnp.where(
        lax.broadcasted_iota(jnp.int32, (heads, width), 0)
        == lax.broadcasted_iota(jnp.int32, (heads, width), 1) // size,
        1.0,
        0.0,
    )
    keys = [k_ref[:, t, :].astype(F32) for t in range(steps)]
    for t in range(steps):
        spread_heads(kscr, keys[t], 0, heads * steps, seqs, heads, steps, size, t)
    pairs = [(t, r) for t in range(steps) for r in range(t + 1)]
    sums = head_sum(jnp.concatenate([keys[t] * keys[r] for t, r in pairs], 0), ones)
    raw = {p: sums[i * seqs : (i + 1) * seqs] for i, p in enumerate(pairs)}
    inv = [lax.rsqrt(raw[t, t] + EPS) for t in range(steps)]

    copies[5].wait()

    def read(s, carry):
        kb = kscr[pl.ds(s * heads * steps, heads * steps), :][:, :size].astype(BF16)
        seen = own_heads(dot(kb, s0_ref[s].astype(BF16)), masks, group, steps)
        put_rows(pscr, s * 8, 8, seen)
        return carry

    lax.fori_loop(0, seqs, read, 0, unroll=8)
    highest = lax.Precision.HIGHEST
    cumul, solved = [], []
    for t in range(steps):
        live = jnp.where(a_ref[...] > t, 1.0, 0.0)
        log = dot(d_ref[t] * live, pick, ((0,), (0,)), highest)
        strength = dot(jax.nn.sigmoid(b_ref[t]) * live, pick, ((0,), (0,)), highest)
        cumul.append(log if t == 0 else cumul[-1] + log)
        seen = get_rows(pscr, t, seqs, 8) * inv[t]
        rest = v_ref[:, t, :].astype(F32) - jnp.exp(cumul[t]) * seen
        for r in range(t):
            rest = rest - jnp.exp(cumul[t] - cumul[r]) * (raw[t, r] * inv[t] * inv[r]) * solved[r]
        solved.append(strength * rest)
    for t in range(steps):
        add = jnp.exp(cumul[-1] - cumul[t]) * inv[t] * solved[t]
        for g in range(group):
            put_rows(uscr, g * steps + t, seqs, add, 8)
    gscr[...] = jnp.exp(cumul[-1])

    def write(s, carry):
        ub = get_rows(uscr, s * 8, 8)
        wide = jnp.concatenate([jnp.where(m, ub, 0.0) for m in masks], 0).astype(BF16)
        kb = kscr[pl.ds(s * heads * steps, heads * steps), :][:, :size].astype(BF16)
        new = gscr[pl.ds(s, 1), :] * s0_ref[s] + dot(kb, wide, ((0,), (0,)))
        out_ref[s] = new
        low_ref[s] = new.astype(BF16)
        return carry

    lax.fori_loop(0, seqs, write, 0, unroll=8)
    for copy in copies[6:]:
        copy.wait()
    if count:
        outs[4][0:1, :] = held[8][...]
        total = None
        for i, ref in enumerate(held[9:11]):
            rows, every = outs[5].shape[0], ref.shape[0]
            row = lax.broadcasted_iota(jnp.int32, (rows, every), 0) - i * heads
            col = lax.broadcasted_iota(jnp.int32, (rows, every), 1)
            chosen = (row >= 0) & (row < heads) & (col == row + lax.axis_index(axes[2]) * heads)
            term = dot(chosen.astype(F32).astype(BF16), ref[...])
            total = term if total is None else total + term
        outs[5][...] = total.astype(BF16)
    entry = jnp.where(
        lax.broadcasted_iota(jnp.int32, (size, width), 0)
        == lax.broadcasted_iota(jnp.int32, (size, width), 1) % size,
        1.0,
        0.0,
    )
    const_ref[0:1, :] = dot(base_ref[...], pick, precision=highest)
    const_ref[1:2, :] = dot(last_ref[...], entry, precision=highest)


def early(axes, state, prev, decay_base, out_gain, shared):
    prev_keys, prev_values, prev_beta, prev_decay, accepted = prev
    seqs, size, width = state.shape
    steps = prev_keys.shape[1]
    heads = width // size
    arrays = (
        prev_keys,
        prev_values,
        jnp.transpose(prev_beta, (1, 2, 0)),
        jnp.transpose(prev_decay, (1, 2, 0)),
        accepted.reshape(1, -1),
        state,
        decay_base.reshape(1, -1),
        out_gain.reshape(1, -1),
    )
    held = [like(a) for a in arrays]
    shapes = [
        jax.ShapeDtypeStruct(state.shape, F32),
        jax.ShapeDtypeStruct(state.shape, BF16),
        jax.ShapeDtypeStruct((8, width), F32),
    ]
    count = 0
    if shared:
        in_gain, w_beta, w_decay, weights, w_out = shared
        count = len(weights)
        rows, columns = weights[0].shape
        arrays += (in_gain.reshape(1, -1), w_beta.T, w_decay.T) + weights + (w_out,)
        small = VMEM((w_beta.shape[1], rows), BF16)
        held += [VMEM((1, rows), F32), small, small]
        shapes += [
            jax.ShapeDtypeStruct((rows, columns * count), BF16),
            jax.ShapeDtypeStruct((8, rows), F32),
            jax.ShapeDtypeStruct((-(-2 * heads // 8) * 8, rows), BF16),
            jax.ShapeDtypeStruct((w_out.shape[0] // 2, w_out.shape[1]), BF16),
        ]
    return pl.pallas_call(
        functools.partial(early_kernel, steps, size, axes, count),
        out_shape=shapes,
        in_specs=[whole(HBM)] * len(arrays),
        out_specs=[whole()] * len(shapes),
        scratch_shapes=held
        + [
            VMEM((seqs * heads * steps, 128), F32),
            VMEM((width // 128, seqs * 8, 128), F32),
            VMEM((width // 128, seqs * 8, 128), F32),
            VMEM((seqs, width), F32),
            pltpu.SemaphoreType.DMA((len(arrays),)),
        ],
        cost_estimate=pl.CostEstimate(
            flops=seqs * 4000000, bytes_accessed=8 * state.size, transcendentals=0
        ),
        compiler_params=limit(20),
        name="early",
    )(*[pltpu.with_memory_space_constraint(a, HBM) for a in arrays])


def propose_kernel(dims, axis, spans, first, seqs, slot, const_ref, s_ref, *refs):
    steps, size, features = dims
    parts = len(spans)
    part_refs, wo, refs = refs[:parts], refs[parts], refs[parts + 1 :]
    stat_in = None if any(sums is not None for _, sums in spans) else refs[0]
    out_refs, (kscr, pscr) = refs[0 if stat_in is None else 1 : -2], refs[-2:]
    width = s_ref.shape[2]
    extra = -(-2 * (width // size) // 8) * 8
    heads = width // size
    group = 8 // steps
    ones = head_ones(width, size)
    masks = [head_mask(g * group, group, steps, width, size) for g in range(heads // group)]
    rows = seqs * steps

    def gathered(starts, count, lanes):
        total = None
        for ref, start in zip(part_refs, starts):
            if start is not None:
                piece = ref[start : start + count, lanes].astype(F32)
                total = piece if total is None else total + piece
        return total

    starts = [start for start, _ in spans]
    if stat_in is None:
        stat = gathered([sums for _, sums in spans], extra, slice(None))
        if slot is not None:
            out_refs[-1][...] = stat
            out_refs = out_refs[:-1]
    else:
        stat = stat_in[...]
    at_slot = 512 * (slot or 0)
    stat = stat[:, at_slot : at_slot + 512]
    logits = stat[:, :128] + stat[:, 128:256]
    total = stat[:, 256:384] + stat[:, 384:]
    flat = jnp.concatenate([logits, total], 0).T[:rows]
    src = lax.broadcasted_iota(jnp.int32, (2 * extra, width), 0)
    head = lax.broadcasted_iota(jnp.int32, (2 * extra, width), 1) // size
    highest = lax.Precision.HIGHEST
    base, gain = const_ref[0:1, :], const_ref[1:2, :]

    def take(row):
        return dot(flat, jnp.where(src == row, 1.0, 0.0), precision=highest)

    scale = lax.rsqrt(take(extra) / features + EPS)
    strength = jax.nn.sigmoid(scale * take(head))
    rate = scale * take(heads + head)
    log = -base * (jnp.maximum(rate, 0.0) + jnp.log1p(jnp.exp(-jnp.abs(rate))))

    def column(w):
        return gathered(starts, rows, slice(w * width, (w + 1) * width)) * scale

    query, key = column(0), column(1)
    squares = head_sum(jnp.concatenate([query * query, key * key], 0), ones)
    query = query * (lax.rsqrt(squares[:rows] + EPS) * size ** (-0.5))
    key = key * lax.rsqrt(squares[rows:] + EPS)

    def at(array, t):
        return array[t * seqs : (t + 1) * seqs]

    stride = 2 * heads * steps
    for t in range(steps):
        spread_heads(kscr, at(query, t), 0, stride, seqs, heads, steps, size, t)
        spread_heads(kscr, at(key, t), heads * steps, stride, seqs, heads, steps, size, t)
    below = [(t, r) for t in range(steps) for r in range(t)]
    inside = [(t, r) for t in range(steps) for r in range(t + 1)]
    products = [at(key, t) * at(key, r) for t, r in below]
    products += [at(query, t) * at(key, r) for t, r in inside]
    sums = head_sum(jnp.concatenate(products, 0), ones)
    k_k = {p: at(sums, i) for i, p in enumerate(below)}
    q_k = {p: at(sums, len(below) + i) for i, p in enumerate(inside)}
    upper = lax.broadcasted_iota(jnp.int32, (8, width), 0) < steps

    def read(s, carry):
        vectors = kscr[pl.ds(s * stride, stride), :][:, :size].astype(BF16)
        seen = dot(vectors, s_ref[first + s])
        half = heads * steps
        from_query = own_heads(seen[:half], masks, group, steps)
        from_key = own_heads(seen[half:], masks, group, steps)
        put_rows(pscr, s * 8, 8, jnp.where(upper, from_query, from_key))
        return carry

    lax.fori_loop(0, seqs, read, 0, unroll=8)
    value, gate = column(2), column(3)
    cumul, solved, outs = [], [], []
    for t in range(steps):
        cumul.append(at(log, t) if t == 0 else cumul[-1] + at(log, t))
        grown = jnp.exp(cumul[t])
        rest = at(value, t) - grown * get_rows(pscr, steps + t, seqs, 8)
        out = grown * get_rows(pscr, t, seqs, 8)
        for r in range(t):
            decay = jnp.exp(cumul[t] - cumul[r])
            rest = rest - decay * k_k[t, r] * solved[r]
            out = out + decay * q_k[t, r] * solved[r]
        solved.append(at(strength, t) * rest)
        outs.append(out + q_k[t, t] * solved[t])
    output = jnp.concatenate(outs, 0)
    mean = head_sum(output * output, ones) * (1.0 / size)
    gated = output * lax.rsqrt(mean + EPS) * gain * (gate / (1.0 + jnp.exp(-gate)))
    gated = gated.astype(BF16)
    n = wo.shape[0]
    tp = lax.axis_index(axis)
    for s in list(range(1, len(out_refs))) + [0]:
        block = wo[lax.bitwise_xor(tp, s)] if n > 1 else wo[0]
        out_refs[s][...] = dot(gated, block).astype(out_refs[s].dtype)


def propose(axis, consts, state, parts, spans, wo, dims, first, seqs, slot, stat):
    steps, size = dims[0], dims[1]
    width = state.shape[2]
    heads = width // size
    rows = seqs * steps
    shapes = [
        jax.ShapeDtypeStruct((rows, wo.shape[2]), F32 if s == 0 and wo.shape[0] > 1 else BF16)
        for s in range(wo.shape[0])
    ]
    inputs = [consts, state, *parts, wo]
    if stat is not None:
        inputs.append(stat)
    elif slot is not None:
        extra = -(-2 * heads // 8) * 8
        shapes.append(jax.ShapeDtypeStruct((extra, parts[0].shape[1]), F32))
    return pl.pallas_call(
        functools.partial(propose_kernel, dims, axis, spans, first, seqs, slot),
        out_shape=shapes,
        in_specs=[whole()] * len(inputs),
        out_specs=[whole()] * len(shapes),
        scratch_shapes=[
            VMEM((seqs * 2 * heads * steps, 128), F32),
            VMEM((width // 128, seqs * 8, 128), F32),
        ],
        compiler_params=limit(12),
        cost_estimate=pl.CostEstimate(
            flops=seqs * 4000000, bytes_accessed=4 * state.size, transcendentals=0
        ),
        name="propose",
    )(*inputs)


def finish_kernel(steps, chunks, *refs):
    ins, out_ref = refs[:-1], refs[-1]
    per = len(ins) // len(chunks)
    for c, (first, each) in enumerate(chunks):
        total = ins[c * per][...].astype(F32)
        for ref in ins[c * per + 1 : (c + 1) * per]:
            total = total + ref[...].astype(F32)
        for t in range(steps):
            out_ref[first : first + each, t, :] = total[t * each : (t + 1) * each].astype(
                out_ref.dtype
            )


def finish(pieces, chunks, seqs, steps):
    flat = [a for piece in pieces for a in piece]
    return pl.pallas_call(
        functools.partial(finish_kernel, steps, chunks),
        out_shape=jax.ShapeDtypeStruct((seqs, steps, flat[0].shape[1]), BF16),
        in_specs=[whole()] * len(flat),
        out_specs=whole(),
        compiler_params=limit(8),
        name="finish",
    )(*flat)


def split(seqs):
    last = max(8, seqs // 4)
    return ((0, seqs - last), (seqs - last, last)) if seqs % 8 == 0 and seqs > 8 else ((0, seqs),)


def body(sizes, *args):
    return layer(sizes, *args)


def layer(
    sizes,
    tokens,
    in_gain,
    w_query,
    w_key,
    w_value,
    w_gate,
    w_beta,
    w_decay,
    decay_base,
    out_gain,
    w_out,
    state,
    prev_keys,
    prev_values,
    prev_beta,
    prev_decay,
    accepted,
):
    n_grp, n_kv, n_tp = sizes
    seqs, steps, _ = tokens.shape
    heads = decay_base.shape[0]
    size = out_gain.shape[0]
    features = in_gain.shape[0]
    dims = (steps, size, features)
    square = n_kv == n_tp and n_kv & (n_kv - 1) == 0 and n_grp == 2
    chunks = split(seqs) if square else ((0, seqs),)
    axes = ("grp", "kv", "tp")
    weights = (w_query, w_key, w_value, w_gate)
    prev = (prev_keys, prev_values, prev_beta, prev_decay, accepted)

    def ring(n, s):
        return [(i, (i + s) % n) for i in range(n)]

    if square:
        n = n_kv
        bits = [n >> i for i in range(1, n.bit_length())]
        turn = [(k * n + t, t * n + (k ^ t)) for k in range(n) for t in range(n)]
        turned = lax.ppermute(tokens, ("kv", "tp"), turn)
    shared = (in_gain, w_beta, w_decay, weights, w_out) if square else None
    new_state, low, consts, *staged = early(axes, state, prev, decay_base, out_gain, shared)
    if square:
        weight, own_gain, small, mine = staged
        turned, weight = lax.optimization_barrier((turned, weight))
        halves, marks = [mine], [0]

        def swap(array, bit):
            return lax.ppermute(array, "kv", [(i, i ^ bit) for i in range(n)])

        halves.append(swap(mine, bits[0]))
        marks.append(bits[0])
        halves.append(swap(mine, bits[1]))
        marks.append(bits[1])
        gathered = lax.all_gather(turned, "tp")
        layout = [
            (i, (c,), c == 0, F32 if i == 0 else BF16) for c in range(len(chunks)) for i in range(n)
        ]
        products = project(gathered, own_gain, weight, small, chunks, layout)
        parts = [list(products[c * n : (c + 1) * n]) for c in range(len(chunks))]
        spans = []
        for c, (first, each) in enumerate(chunks):
            for i in range(1, n):
                parts[c][i] = swap(parts[c][i], i)
            spans.append([(0, each * steps if c == 0 else None)] * n)
        halves, parts[0][0] = lax.optimization_barrier((halves, parts[0][0]))
        for bit in bits[1:]:
            for j in range(len(halves)):
                if marks[j] ^ bit not in marks:
                    halves.append(swap(halves[j], bit))
                    marks.append(marks[j] ^ bit)
        arrays, blocks = [w_out], [(0, None)]
        for i in range(1, len(halves)):
            other = lax.ppermute(halves[i], "grp", ring(n_grp, 1))
            arrays += [halves[i], other]
            blocks += [(marks[i], 0), (marks[i], 1)]
        wo = assemble(axes, arrays, blocks, n)
    else:
        x = lax.all_gather(tokens, "tp", axis=2, tiled=True)
        x = jnp.transpose(x, (1, 0, 2)).reshape(seqs * steps, -1).astype(F32)
        square_sum = jnp.sum(x * x, -1)
        x = (x * in_gain).astype(BF16)
        full = [lax.all_gather(w, "kv", axis=0, tiled=True) for w in weights]
        products = [jnp.dot(x, w, preferred_element_type=F32) for w in full]
        start = lax.axis_index("tp") * heads
        chosen = [lax.dynamic_slice_in_dim(w, start, heads, 1) for w in (w_beta, w_decay)]
        logits = jnp.dot(x, jnp.concatenate(chosen, 1), preferred_element_type=F32).T
        extra = -(-2 * heads // 8) * 8
        sums = jnp.zeros((extra, sum(p.shape[1] for p in products)), F32)
        sums = sums.at[: 2 * heads, : seqs * steps].set(logits)
        sums = sums.at[0, 256 : 256 + seqs * steps].set(square_sum)
        parts = [[jnp.concatenate([jnp.concatenate(products, 1), sums], 0)]]
        spans = [[(0, seqs * steps)]]
        wo = lax.all_gather(w_out, "kv", axis=1, tiled=True)[None]

    pieces, stat = [], None
    for c, (first, each) in enumerate(chunks):
        slot = c if len(chunks) > 1 else None
        out = propose(
            "tp", consts, low, parts[c], spans[c], wo, dims, first, each, slot, stat
        )
        if slot == 0:
            stat = out[-1]
        if square:
            pieces.append(
                [out[0]]
                + [
                    lax.ppermute(out[s], "tp", [(i, i ^ s) for i in range(n_tp)])
                    for s in range(1, n_tp)
                ]
            )
        else:
            pieces.append([lax.psum_scatter(out[0], "tp", scatter_dimension=1, tiled=True)])
    return finish(pieces, chunks, seqs, steps), new_state


def solution(mesh):
    rows = P(("grp", "kv"), None, "tp")
    matrix = P("kv", "tp")
    placed = (
        rows,
        P(),
        matrix,
        matrix,
        matrix,
        matrix,
        P(),
        P(),
        P("tp"),
        P(),
        P("tp", "kv"),
        rows,
        rows,
        rows,
        rows,
        rows,
        P(("grp", "kv")),
    )
    sizes = (mesh.shape["grp"], mesh.shape["kv"], mesh.shape["tp"])
    return jax.shard_map(
        functools.partial(body, sizes),
        mesh=mesh,
        in_specs=placed,
        out_specs=(rows, rows),
        check_vma=False,
    )
```

```python
import functools

import jax
import jax.numpy as jnp
from jax import lax
from jax.experimental import pallas as pl
from jax.experimental.pallas import tpu as pltpu
from jax.sharding import PartitionSpec as P

EPS = 1e-06
F32 = jnp.float32
BF16 = jnp.bfloat16
VMEM = pltpu.VMEM
HBM = pltpu.HBM


def whole(space=VMEM):
    return pl.BlockSpec(memory_space=space)


def fetch(sources, targets, sems):
    copies = [
        pltpu.make_async_copy(source, target, sems.at[i])
        for i, (source, target) in enumerate(zip(sources, targets))
    ]
    for copy in copies:
        copy.start()
    return copies


def like(array):
    return VMEM(array.shape, array.dtype)


def limit(mebibytes):
    return pltpu.CompilerParams(vmem_limit_bytes=mebibytes << 20)


def dot(a, b, contract=((1,), (0,)), precision=None):
    return lax.dot_general(
        a, b, (contract, ((), ())), precision=precision, preferred_element_type=F32
    )


def head_ones(width, size):
    row = lax.broadcasted_iota(jnp.int32, (width, width), 0) // size
    col = lax.broadcasted_iota(jnp.int32, (width, width), 1) // size
    return jnp.where(row == col, 1.0, 0.0).astype(BF16)


def head_sum(values, ones):
    high = values.astype(BF16)
    low = (values - high.astype(F32)).astype(BF16)
    return dot(high, ones) + dot(low, ones)


def head_mask(first, group, steps, width, size):
    sub = lax.broadcasted_iota(jnp.int32, (group * steps, width), 0) // steps + first
    lane = lax.broadcasted_iota(jnp.int32, (group * steps, width), 1) // size
    return sub == lane


def block_of(axis, size):
    return pl.ds(pl.multiple_of(lax.axis_index(axis) * size, size), size)


def stat_rows(values):
    high = values.astype(BF16).astype(F32)
    return high, values - high


def project_kernel(chunks, layout, x_ref, gain_ref, weight_ref, small_ref, *outs):
    _, _, steps, local = x_ref.shape
    gain = gain_ref[0:1, :]
    raw, spans, start = [], {}, 0
    for d in sorted({d for d, _, _ in layout}):
        tokens = [x_ref[d, :, t, :].astype(F32) for t in range(steps)]
        for c, (first, each) in enumerate(chunks):
            raw += [x[first : first + each] for x in tokens]
            spans[d, c] = slice(start, start + each * steps)
            start += each * steps
    raw = jnp.concatenate(raw, 0)
    x = (raw * gain).astype(BF16)
    square = raw * raw
    high = square.astype(BF16)
    low = (square - high.astype(F32)).astype(BF16)
    count = small_ref.shape[0]
    unit = (lax.broadcasted_iota(jnp.int32, (128, local), 0) == count).astype(F32).astype(BF16)
    small = jnp.concatenate([small_ref[...], jnp.zeros((128 - count, local), BF16)], 0)
    sums = dot(x, small, ((1,), (1,))) + dot(high, unit, ((1,), (1,))) + dot(low, unit, ((1,), (1,)))
    width = weight_ref.shape[1]
    for out, (d, parts, with_sums) in zip(outs, layout):
        if not with_sums:
            continue
        extra = []
        for c in range(len(chunks)):
            part = sums[spans[d, c]]
            if part.shape[0] < 128:
                part = jnp.concatenate([part, jnp.zeros((128 - part.shape[0], 128), F32)], 0)
            part = part.T
            for first in range(0, 2 * count, count):
                extra += stat_rows(part[first : first + count])
        if width > 128 * len(extra):
            extra.append(jnp.zeros((count, width - 128 * len(extra)), F32))
        out[out.shape[0] - count :, :] = jnp.concatenate(extra, 1).astype(out.dtype)
    block = min(width, 256)
    for first in range(0, width, block):
        lanes = slice(first, first + block)
        product = dot(x, weight_ref[:, lanes])
        for out, (d, parts, _) in zip(outs, layout):
            start = 0
            for c in parts:
                piece = product[spans[d, c]]
                out[start : start + piece.shape[0], lanes] = piece.astype(out.dtype)
                start += piece.shape[0]


def project(x, gain, weight, small, chunks, layout):
    _, _, steps, _ = x.shape
    width = weight.shape[1]

    def shape(d, parts, with_sums, dtype):
        rows = sum(chunks[c][1] for c in parts) * steps
        return jax.ShapeDtypeStruct((rows + small.shape[0] * with_sums, width), dtype)

    return pl.pallas_call(
        functools.partial(project_kernel, chunks, [entry[:3] for entry in layout]),
        out_shape=[shape(*entry) for entry in layout],
        in_specs=[whole()] * 4,
        out_specs=[whole()] * len(layout),
        compiler_params=limit(16),
        cost_estimate=pl.CostEstimate(
            flops=2 * x.size * width, bytes_accessed=4 * x.size, transcendentals=0
        ),
    )(x, gain, weight, small)


def assemble_kernel(axes, blocks, *refs):
    sources, out_ref, sems = refs[:-2], refs[-2], refs[-1]
    place = [lax.axis_index(axis) for axis in axes]
    targets = []
    for ref, (mark, flip) in zip(sources, blocks):
        target = out_ref.at[lax.bitwise_xor(place[1], mark)]
        if flip is not None:
            count = ref.shape[0]
            row = lax.bitwise_xor(place[0], flip) * count
            target = target.at[pl.ds(pl.multiple_of(row, count), count)]
        targets.append(target)
    for copy in fetch(sources, targets, sems):
        copy.wait()


def assemble(axes, arrays, blocks, n):
    return pl.pallas_call(
        functools.partial(assemble_kernel, axes, blocks),
        out_shape=jax.ShapeDtypeStruct((n,) + arrays[0].shape, arrays[0].dtype),
        in_specs=[whole(HBM)] * len(arrays),
        out_specs=whole(),
        scratch_shapes=[pltpu.SemaphoreType.DMA((len(arrays),))],
        compiler_params=limit(4),
        cost_estimate=pl.CostEstimate(
            flops=4000000, bytes_accessed=8 * arrays[0].size, transcendentals=0
        ),
        name="assemble",
    )(*arrays)


def spread_heads(ref, value, offset, stride, seqs, heads, steps, size, t):
    for h in range(heads):
        tile, lane = divmod(h * size, 128)
        part = value[:, tile * 128 : (tile + 1) * 128]
        if lane:
            part = pltpu.roll(part, 128 - lane, 1)
        ref[pl.ds(offset + h * steps + t, seqs, stride=stride), :] = part


def put_rows(ref, start, count, value, stride=None):
    for m in range(ref.shape[0]):
        ref[m, pl.ds(start, count, stride=stride), :] = value[:, m * 128 : (m + 1) * 128]


def get_rows(ref, start, count, stride=None):
    return jnp.concatenate(
        [ref[m, pl.ds(start, count, stride=stride), :] for m in range(ref.shape[0])], 1
    )


def own_heads(product, masks, group, steps):
    tile = group * steps
    total = None
    for m, mask in enumerate(masks):
        part = jnp.where(mask, product[m * tile : (m + 1) * tile], 0.0)
        total = part if total is None else total + part
    shift = steps
    acc = total
    for _ in range(group - 1):
        acc = acc + pltpu.roll(total, shift, 0)
        shift += steps
    return acc


def early_kernel(steps, size, axes, count, *refs):
    inputs = 12 + count if count else 8
    own = 11 if count else 8
    sources, refs = refs[:inputs], refs[inputs:]
    outputs = 7 if count else 3
    outs, refs = refs[:outputs], refs[outputs:]
    out_ref, low_ref, const_ref = outs[:3]
    held, (kscr, pscr, uscr, gscr, sems) = refs[:own], refs[own:]
    k_ref, v_ref, b_ref, d_ref, a_ref, s0_ref = held[:6]
    base_ref, last_ref = held[6:8]
    seqs, _, width = s0_ref.shape
    views = list(sources[:8])
    if count:
        part = block_of(axes[1], held[8].shape[1])
        views += [ref.at[:, part] for ref in sources[8:11]]
    copies = fetch(views, held, sems)
    if count:
        half = sources[-1].at[block_of(axes[0], outs[6].shape[0])]
        wide = sources[11].shape[1]
        targets = [outs[3].at[:, i * wide : (i + 1) * wide] for i in range(count)]
        copies += fetch(
            [half] + list(sources[11:-1]), [outs[6]] + targets, sems.at[pl.ds(11, count + 1)]
        )
    for copy in copies[:5]:
        copy.wait()
    heads = width // size
    group = 8 // steps
    ones = head_ones(width, size)
    masks = [head_mask(g * group, group, steps, width, size) for g in range(heads // group)]
    pick = jnp.where(
        lax.broadcasted_iota(jnp.int32, (heads, width), 0)
        == lax.broadcasted_iota(jnp.int32, (heads, width), 1) // size,
        1.0,
        0.0,
    )
    keys = [k_ref[:, t, :].astype(F32) for t in range(steps)]
    for t in range(steps):
        spread_heads(kscr, keys[t], 0, heads * steps, seqs, heads, steps, size, t)
    pairs = [(t, r) for t in range(steps) for r in range(t + 1)]
    sums = head_sum(jnp.concatenate([keys[t] * keys[r] for t, r in pairs], 0), ones)
    raw = {p: sums[i * seqs : (i + 1) * seqs] for i, p in enumerate(pairs)}
    inv = [lax.rsqrt(raw[t, t] + EPS) for t in range(steps)]

    copies[5].wait()

    def read(s, carry):
        kb = kscr[pl.ds(s * heads * steps, heads * steps), :][:, :size].astype(BF16)
        seen = own_heads(dot(kb, s0_ref[s].astype(BF16)), masks, group, steps)
        put_rows(pscr, s * 8, 8, seen)
        return carry

    lax.fori_loop(0, seqs, read, 0, unroll=8)
    highest = lax.Precision.HIGHEST
    cumul, solved = [], []
    for t in range(steps):
        live = jnp.where(a_ref[...] > t, 1.0, 0.0)
        log = dot(d_ref[t] * live, pick, ((0,), (0,)), highest)
        strength = dot(jax.nn.sigmoid(b_ref[t]) * live, pick, ((0,), (0,)), highest)
        cumul.append(log if t == 0 else cumul[-1] + log)
        seen = get_rows(pscr, t, seqs, 8) * inv[t]
        rest = v_ref[:, t, :].astype(F32) - jnp.exp(cumul[t]) * seen
        for r in range(t):
            rest = rest - jnp.exp(cumul[t] - cumul[r]) * (raw[t, r] * inv[t] * inv[r]) * solved[r]
        solved.append(strength * rest)
    for t in range(steps):
        add = jnp.exp(cumul[-1] - cumul[t]) * inv[t] * solved[t]
        for g in range(group):
            put_rows(uscr, g * steps + t, seqs, add, 8)
    gscr[...] = jnp.exp(cumul[-1])

    def write(s, carry):
        ub = get_rows(uscr, s * 8, 8)
        wide = jnp.concatenate([jnp.where(m, ub, 0.0) for m in masks], 0).astype(BF16)
        kb = kscr[pl.ds(s * heads * steps, heads * steps), :][:, :size].astype(BF16)
        new = gscr[pl.ds(s, 1), :] * s0_ref[s] + dot(kb, wide, ((0,), (0,)))
        out_ref[s] = new
        low_ref[s] = new.astype(BF16)
        return carry

    lax.fori_loop(0, seqs, write, 0, unroll=8)
    for copy in copies[6:]:
        copy.wait()
    if count:
        outs[4][0:1, :] = held[8][...]
        total = None
        for i, ref in enumerate(held[9:11]):
            rows, every = outs[5].shape[0], ref.shape[0]
            row = lax.broadcasted_iota(jnp.int32, (rows, every), 0) - i * heads
            col = lax.broadcasted_iota(jnp.int32, (rows, every), 1)
            chosen = (row >= 0) & (row < heads) & (col == row + lax.axis_index(axes[2]) * heads)
            term = dot(chosen.astype(F32).astype(BF16), ref[...])
            total = term if total is None else total + term
        outs[5][...] = total.astype(BF16)
    entry = jnp.where(
        lax.broadcasted_iota(jnp.int32, (size, width), 0)
        == lax.broadcasted_iota(jnp.int32, (size, width), 1) % size,
        1.0,
        0.0,
    )
    const_ref[0:1, :] = dot(base_ref[...], pick, precision=highest)
    const_ref[1:2, :] = dot(last_ref[...], entry, precision=highest)


def early(axes, state, prev, decay_base, out_gain, shared):
    prev_keys, prev_values, prev_beta, prev_decay, accepted = prev
    seqs, size, width = state.shape
    steps = prev_keys.shape[1]
    heads = width // size
    arrays = (
        prev_keys,
        prev_values,
        jnp.transpose(prev_beta, (1, 2, 0)),
        jnp.transpose(prev_decay, (1, 2, 0)),
        accepted.reshape(1, -1),
        state,
        decay_base.reshape(1, -1),
        out_gain.reshape(1, -1),
    )
    held = [like(a) for a in arrays]
    shapes = [
        jax.ShapeDtypeStruct(state.shape, F32),
        jax.ShapeDtypeStruct(state.shape, BF16),
        jax.ShapeDtypeStruct((8, width), F32),
    ]
    count = 0
    if shared:
        in_gain, w_beta, w_decay, weights, w_out = shared
        count = len(weights)
        rows, columns = weights[0].shape
        arrays += (in_gain.reshape(1, -1), w_beta.T, w_decay.T) + weights + (w_out,)
        small = VMEM((w_beta.shape[1], rows), BF16)
        held += [VMEM((1, rows), F32), small, small]
        shapes += [
            jax.ShapeDtypeStruct((rows, columns * count), BF16),
            jax.ShapeDtypeStruct((8, rows), F32),
            jax.ShapeDtypeStruct((-(-2 * heads // 8) * 8, rows), BF16),
            jax.ShapeDtypeStruct((w_out.shape[0] // 2, w_out.shape[1]), BF16),
        ]
    return pl.pallas_call(
        functools.partial(early_kernel, steps, size, axes, count),
        out_shape=shapes,
        in_specs=[whole(HBM)] * len(arrays),
        out_specs=[whole()] * len(shapes),
        scratch_shapes=held
        + [
            VMEM((seqs * heads * steps, 128), F32),
            VMEM((width // 128, seqs * 8, 128), F32),
            VMEM((width // 128, seqs * 8, 128), F32),
            VMEM((seqs, width), F32),
            pltpu.SemaphoreType.DMA((len(arrays),)),
        ],
        cost_estimate=pl.CostEstimate(
            flops=seqs * 4000000, bytes_accessed=8 * state.size, transcendentals=0
        ),
        compiler_params=limit(20),
        name="early",
    )(*[pltpu.with_memory_space_constraint(a, HBM) for a in arrays])


def propose_kernel(dims, axis, spans, first, seqs, slot, const_ref, s_ref, *refs):
    steps, size, features = dims
    parts = len(spans)
    part_refs, wo, refs = refs[:parts], refs[parts], refs[parts + 1 :]
    stat_in = None if any(sums is not None for _, sums in spans) else refs[0]
    out_refs, (kscr, pscr) = refs[0 if stat_in is None else 1 : -2], refs[-2:]
    width = s_ref.shape[2]
    extra = -(-2 * (width // size) // 8) * 8
    heads = width // size
    group = 8 // steps
    ones = head_ones(width, size)
    masks = [head_mask(g * group, group, steps, width, size) for g in range(heads // group)]
    rows = seqs * steps

    def gathered(starts, count, lanes):
        total = None
        for ref, start in zip(part_refs, starts):
            if start is not None:
                piece = ref[start : start + count, lanes].astype(F32)
                total = piece if total is None else total + piece
        return total

    starts = [start for start, _ in spans]
    if stat_in is None:
        stat = gathered([sums for _, sums in spans], extra, slice(None))
        if slot is not None:
            out_refs[-1][...] = stat
            out_refs = out_refs[:-1]
    else:
        stat = stat_in[...]
    at_slot = 512 * (slot or 0)
    stat = stat[:, at_slot : at_slot + 512]
    logits = stat[:, :128] + stat[:, 128:256]
    total = stat[:, 256:384] + stat[:, 384:]
    flat = jnp.concatenate([logits, total], 0).T[:rows]
    src = lax.broadcasted_iota(jnp.int32, (2 * extra, width), 0)
    head = lax.broadcasted_iota(jnp.int32, (2 * extra, width), 1) // size
    highest = lax.Precision.HIGHEST
    base, gain = const_ref[0:1, :], const_ref[1:2, :]

    def take(row):
        return dot(flat, jnp.where(src == row, 1.0, 0.0), precision=highest)

    scale = lax.rsqrt(take(extra) / features + EPS)
    strength = jax.nn.sigmoid(scale * take(head))
    rate = scale * take(heads + head)
    log = -base * (jnp.maximum(rate, 0.0) + jnp.log1p(jnp.exp(-jnp.abs(rate))))

    def column(w):
        return gathered(starts, rows, slice(w * width, (w + 1) * width)) * scale

    query, key = column(0), column(1)
    squares = head_sum(jnp.concatenate([query * query, key * key], 0), ones)
    query = query * (lax.rsqrt(squares[:rows] + EPS) * size ** (-0.5))
    key = key * lax.rsqrt(squares[rows:] + EPS)

    def at(array, t):
        return array[t * seqs : (t + 1) * seqs]

    stride = 2 * heads * steps
    for t in range(steps):
        spread_heads(kscr, at(query, t), 0, stride, seqs, heads, steps, size, t)
        spread_heads(kscr, at(key, t), heads * steps, stride, seqs, heads, steps, size, t)
    below = [(t, r) for t in range(steps) for r in range(t)]
    inside = [(t, r) for t in range(steps) for r in range(t + 1)]
    products = [at(key, t) * at(key, r) for t, r in below]
    products += [at(query, t) * at(key, r) for t, r in inside]
    sums = head_sum(jnp.concatenate(products, 0), ones)
    k_k = {p: at(sums, i) for i, p in enumerate(below)}
    q_k = {p: at(sums, len(below) + i) for i, p in enumerate(inside)}
    upper = lax.broadcasted_iota(jnp.int32, (8, width), 0) < steps

    def read(s, carry):
        vectors = kscr[pl.ds(s * stride, stride), :][:, :size].astype(BF16)
        seen = dot(vectors, s_ref[first + s])
        half = heads * steps
        from_query = own_heads(seen[:half], masks, group, steps)
        from_key = own_heads(seen[half:], masks, group, steps)
        put_rows(pscr, s * 8, 8, jnp.where(upper, from_query, from_key))
        return carry

    lax.fori_loop(0, seqs, read, 0, unroll=8)
    value, gate = column(2), column(3)
    cumul, solved, outs = [], [], []
    for t in range(steps):
        cumul.append(at(log, t) if t == 0 else cumul[-1] + at(log, t))
        grown = jnp.exp(cumul[t])
        rest = at(value, t) - grown * get_rows(pscr, steps + t, seqs, 8)
        out = grown * get_rows(pscr, t, seqs, 8)
        for r in range(t):
            decay = jnp.exp(cumul[t] - cumul[r])
            rest = rest - decay * k_k[t, r] * solved[r]
            out = out + decay * q_k[t, r] * solved[r]
        solved.append(at(strength, t) * rest)
        outs.append(out + q_k[t, t] * solved[t])
    output = jnp.concatenate(outs, 0)
    mean = head_sum(output * output, ones) * (1.0 / size)
    gated = output * lax.rsqrt(mean + EPS) * gain * (gate / (1.0 + jnp.exp(-gate)))
    gated = gated.astype(BF16)
    n = wo.shape[0]
    tp = lax.axis_index(axis)
    for s in list(range(1, len(out_refs))) + [0]:
        block = wo[lax.bitwise_xor(tp, s)] if n > 1 else wo[0]
        out_refs[s][...] = dot(gated, block).astype(out_refs[s].dtype)


def propose(axis, consts, state, parts, spans, wo, dims, first, seqs, slot, stat):
    steps, size = dims[0], dims[1]
    width = state.shape[2]
    heads = width // size
    rows = seqs * steps
    shapes = [
        jax.ShapeDtypeStruct((rows, wo.shape[2]), F32 if s == 0 and wo.shape[0] > 1 else BF16)
        for s in range(wo.shape[0])
    ]
    inputs = [consts, state, *parts, wo]
    if stat is not None:
        inputs.append(stat)
    elif slot is not None:
        extra = -(-2 * heads // 8) * 8
        shapes.append(jax.ShapeDtypeStruct((extra, parts[0].shape[1]), F32))
    return pl.pallas_call(
        functools.partial(propose_kernel, dims, axis, spans, first, seqs, slot),
        out_shape=shapes,
        in_specs=[whole()] * len(inputs),
        out_specs=[whole()] * len(shapes),
        scratch_shapes=[
            VMEM((seqs * 2 * heads * steps, 128), F32),
            VMEM((width // 128, seqs * 8, 128), F32),
        ],
        compiler_params=limit(12),
        cost_estimate=pl.CostEstimate(
            flops=seqs * 4000000, bytes_accessed=4 * state.size, transcendentals=0
        ),
        name="propose",
    )(*inputs)


def finish_kernel(steps, chunks, *refs):
    ins, out_ref = refs[:-1], refs[-1]
    per = len(ins) // len(chunks)
    for c, (first, each) in enumerate(chunks):
        total = ins[c * per][...].astype(F32)
        for ref in ins[c * per + 1 : (c + 1) * per]:
            total = total + ref[...].astype(F32)
        for t in range(steps):
            out_ref[first : first + each, t, :] = total[t * each : (t + 1) * each].astype(
                out_ref.dtype
            )


def finish(pieces, chunks, seqs, steps):
    flat = [a for piece in pieces for a in piece]
    return pl.pallas_call(
        functools.partial(finish_kernel, steps, chunks),
        out_shape=jax.ShapeDtypeStruct((seqs, steps, flat[0].shape[1]), BF16),
        in_specs=[whole()] * len(flat),
        out_specs=whole(),
        compiler_params=limit(8),
        name="finish",
    )(*flat)


def split(seqs):
    last = max(8, seqs // 4)
    return ((0, seqs - last), (seqs - last, last)) if seqs % 8 == 0 and seqs > 8 else ((0, seqs),)


def body(sizes, *args):
    return layer(sizes, *args)


def layer(
    sizes,
    tokens,
    in_gain,
    w_query,
    w_key,
    w_value,
    w_gate,
    w_beta,
    w_decay,
    decay_base,
    out_gain,
    w_out,
    state,
    prev_keys,
    prev_values,
    prev_beta,
    prev_decay,
    accepted,
):
    n_grp, n_kv, n_tp = sizes
    seqs, steps, _ = tokens.shape
    heads = decay_base.shape[0]
    size = out_gain.shape[0]
    features = in_gain.shape[0]
    dims = (steps, size, features)
    square = n_kv == n_tp and n_kv & (n_kv - 1) == 0 and n_grp == 2
    chunks = split(seqs) if square else ((0, seqs),)
    axes = ("grp", "kv", "tp")
    weights = (w_query, w_key, w_value, w_gate)
    prev = (prev_keys, prev_values, prev_beta, prev_decay, accepted)

    def ring(n, s):
        return [(i, (i + s) % n) for i in range(n)]

    if square:
        n = n_kv
        bits = [n >> i for i in range(1, n.bit_length())]
        turn = [(k * n + t, t * n + (k ^ t)) for k in range(n) for t in range(n)]
        turned = lax.ppermute(tokens, ("kv", "tp"), turn)
    shared = (in_gain, w_beta, w_decay, weights, w_out) if square else None
    new_state, low, consts, *staged = early(axes, state, prev, decay_base, out_gain, shared)
    if square:
        weight, own_gain, small, mine = staged
        turned, weight = lax.optimization_barrier((turned, weight))
        halves, marks = [mine], [0]

        def swap(array, bit):
            return lax.ppermute(array, "kv", [(i, i ^ bit) for i in range(n)])

        halves.append(swap(mine, bits[0]))
        marks.append(bits[0])
        halves.append(swap(mine, bits[1]))
        marks.append(bits[1])
        gathered = lax.all_gather(turned, "tp")
        parts = [[None] * n for _ in chunks]
        rest = [i for i in range(n) if i != bits[0]]
        for owners in ([bits[0]], rest):
            layout = [
                (i, (c,), c == 0, F32 if i == 0 else BF16)
                for c in range(len(chunks))
                for i in owners
            ]
            products = project(gathered, own_gain, weight, small, chunks, layout)
            for (i, (c,), _, _), product in zip(layout, products):
                parts[c][i] = product
        spans = []
        for c, (first, each) in enumerate(chunks):
            for i in range(1, n):
                parts[c][i] = swap(parts[c][i], i)
            spans.append([(0, each * steps if c == 0 else None)] * n)
        halves, parts[0][0] = lax.optimization_barrier((halves, parts[0][0]))
        for bit in bits[1:]:
            for j in range(len(halves)):
                if marks[j] ^ bit not in marks:
                    halves.append(swap(halves[j], bit))
                    marks.append(marks[j] ^ bit)
        arrays, blocks = [w_out], [(0, None)]
        for i in range(1, len(halves)):
            other = lax.ppermute(halves[i], "grp", ring(n_grp, 1))
            arrays += [halves[i], other]
            blocks += [(marks[i], 0), (marks[i], 1)]
        wo = assemble(axes, arrays, blocks, n)
    else:
        x = lax.all_gather(tokens, "tp", axis=2, tiled=True)
        x = jnp.transpose(x, (1, 0, 2)).reshape(seqs * steps, -1).astype(F32)
        square_sum = jnp.sum(x * x, -1)
        x = (x * in_gain).astype(BF16)
        full = [lax.all_gather(w, "kv", axis=0, tiled=True) for w in weights]
        products = [jnp.dot(x, w, preferred_element_type=F32) for w in full]
        start = lax.axis_index("tp") * heads
        chosen = [lax.dynamic_slice_in_dim(w, start, heads, 1) for w in (w_beta, w_decay)]
        logits = jnp.dot(x, jnp.concatenate(chosen, 1), preferred_element_type=F32).T
        extra = -(-2 * heads // 8) * 8
        sums = jnp.zeros((extra, sum(p.shape[1] for p in products)), F32)
        sums = sums.at[: 2 * heads, : seqs * steps].set(logits)
        sums = sums.at[0, 256 : 256 + seqs * steps].set(square_sum)
        parts = [[jnp.concatenate([jnp.concatenate(products, 1), sums], 0)]]
        spans = [[(0, seqs * steps)]]
        wo = lax.all_gather(w_out, "kv", axis=1, tiled=True)[None]

    pieces, stat = [], None
    for c, (first, each) in enumerate(chunks):
        slot = c if len(chunks) > 1 else None
        out = propose(
            "tp", consts, low, parts[c], spans[c], wo, dims, first, each, slot, stat
        )
        if slot == 0:
            stat = out[-1]
        if square:
            pieces.append(
                [out[0]]
                + [
                    lax.ppermute(out[s], "tp", [(i, i ^ s) for i in range(n_tp)])
                    for s in range(1, n_tp)
                ]
            )
        else:
            pieces.append([lax.psum_scatter(out[0], "tp", scatter_dimension=1, tiled=True)])
    return finish(pieces, chunks, seqs, steps), new_state


def solution(mesh):
    rows = P(("grp", "kv"), None, "tp")
    matrix = P("kv", "tp")
    placed = (
        rows,
        P(),
        matrix,
        matrix,
        matrix,
        matrix,
        P(),
        P(),
        P("tp"),
        P(),
        P("tp", "kv"),
        rows,
        rows,
        rows,
        rows,
        rows,
        P(("grp", "kv")),
    )
    sizes = (mesh.shape["grp"], mesh.shape["kv"], mesh.shape["tp"])
    return jax.shard_map(
        functools.partial(body, sizes),
        mesh=mesh,
        in_specs=placed,
        out_specs=(rows, rows),
        check_vma=False,
    )
```

```python
import functools

import jax
import jax.numpy as jnp
from jax import lax
from jax.experimental import pallas as pl
from jax.experimental.pallas import tpu as pltpu
from jax.sharding import PartitionSpec as P

EPS = 1e-06
F32 = jnp.float32
BF16 = jnp.bfloat16
VMEM = pltpu.VMEM
HBM = pltpu.HBM


def whole(space=VMEM):
    return pl.BlockSpec(memory_space=space)


def fetch(sources, targets, sems):
    copies = [
        pltpu.make_async_copy(source, target, sems.at[i])
        for i, (source, target) in enumerate(zip(sources, targets))
    ]
    for copy in copies:
        copy.start()
    return copies


def like(array):
    return VMEM(array.shape, array.dtype)


def limit(mebibytes):
    return pltpu.CompilerParams(vmem_limit_bytes=mebibytes << 20)


def dot(a, b, contract=((1,), (0,)), precision=None):
    return lax.dot_general(
        a, b, (contract, ((), ())), precision=precision, preferred_element_type=F32
    )


def head_ones(width, size):
    row = lax.broadcasted_iota(jnp.int32, (width, width), 0) // size
    col = lax.broadcasted_iota(jnp.int32, (width, width), 1) // size
    return jnp.where(row == col, 1.0, 0.0).astype(BF16)


def head_sum(values, ones):
    high = values.astype(BF16)
    low = (values - high.astype(F32)).astype(BF16)
    return dot(high, ones) + dot(low, ones)


def head_mask(first, group, steps, width, size):
    sub = lax.broadcasted_iota(jnp.int32, (group * steps, width), 0) // steps + first
    lane = lax.broadcasted_iota(jnp.int32, (group * steps, width), 1) // size
    return sub == lane


def block_of(axis, size):
    return pl.ds(pl.multiple_of(lax.axis_index(axis) * size, size), size)


def stat_rows(values):
    high = values.astype(BF16).astype(F32)
    return high, values - high


def project_kernel(chunks, layout, x_ref, gain_ref, weight_ref, small_ref, *outs):
    _, _, steps, local = x_ref.shape
    gain = gain_ref[0:1, :]
    raw, spans, start = [], {}, 0
    for d in sorted({d for d, _, _ in layout}):
        tokens = [x_ref[d, :, t, :].astype(F32) for t in range(steps)]
        for c, (first, each) in enumerate(chunks):
            raw += [x[first : first + each] for x in tokens]
            spans[d, c] = slice(start, start + each * steps)
            start += each * steps
    raw = jnp.concatenate(raw, 0)
    x = (raw * gain).astype(BF16)
    square = raw * raw
    high = square.astype(BF16)
    low = (square - high.astype(F32)).astype(BF16)
    count = small_ref.shape[0]
    unit = (lax.broadcasted_iota(jnp.int32, (128, local), 0) == count).astype(F32).astype(BF16)
    small = jnp.concatenate([small_ref[...], jnp.zeros((128 - count, local), BF16)], 0)
    sums = dot(x, small, ((1,), (1,))) + dot(high, unit, ((1,), (1,))) + dot(low, unit, ((1,), (1,)))
    width = weight_ref.shape[1]
    for out, (d, parts, with_sums) in zip(outs, layout):
        if not with_sums:
            continue
        extra = []
        for c in range(len(chunks)):
            part = sums[spans[d, c]]
            if part.shape[0] < 128:
                part = jnp.concatenate([part, jnp.zeros((128 - part.shape[0], 128), F32)], 0)
            part = part.T
            for first in range(0, 2 * count, count):
                extra += stat_rows(part[first : first + count])
        if width > 128 * len(extra):
            extra.append(jnp.zeros((count, width - 128 * len(extra)), F32))
        out[out.shape[0] - count :, :] = jnp.concatenate(extra, 1).astype(out.dtype)
    block = min(width, 256)
    for first in range(0, width, block):
        lanes = slice(first, first + block)
        product = dot(x, weight_ref[:, lanes])
        for out, (d, parts, _) in zip(outs, layout):
            start = 0
            for c in parts:
                piece = product[spans[d, c]]
                out[start : start + piece.shape[0], lanes] = piece.astype(out.dtype)
                start += piece.shape[0]


def project(x, gain, weight, small, chunks, layout):
    _, _, steps, _ = x.shape
    width = weight.shape[1]

    def shape(d, parts, with_sums, dtype):
        rows = sum(chunks[c][1] for c in parts) * steps
        return jax.ShapeDtypeStruct((rows + small.shape[0] * with_sums, width), dtype)

    return pl.pallas_call(
        functools.partial(project_kernel, chunks, [entry[:3] for entry in layout]),
        out_shape=[shape(*entry) for entry in layout],
        in_specs=[whole()] * 4,
        out_specs=[whole()] * len(layout),
        compiler_params=limit(16),
        cost_estimate=pl.CostEstimate(
            flops=2 * x.size * width, bytes_accessed=4 * x.size, transcendentals=0
        ),
    )(x, gain, weight, small)


def assemble_kernel(axes, blocks, *refs):
    sources, out_ref, sems = refs[:-2], refs[-2], refs[-1]
    place = [lax.axis_index(axis) for axis in axes]
    targets = []
    for ref, (mark, flip) in zip(sources, blocks):
        target = out_ref.at[lax.bitwise_xor(place[1], mark)]
        if flip is not None:
            count = ref.shape[0]
            row = lax.bitwise_xor(place[0], flip) * count
            target = target.at[pl.ds(pl.multiple_of(row, count), count)]
        targets.append(target)
    for copy in fetch(sources, targets, sems):
        copy.wait()


def assemble(axes, arrays, blocks, n):
    return pl.pallas_call(
        functools.partial(assemble_kernel, axes, blocks),
        out_shape=jax.ShapeDtypeStruct((n,) + arrays[0].shape, arrays[0].dtype),
        in_specs=[whole(HBM)] * len(arrays),
        out_specs=whole(),
        scratch_shapes=[pltpu.SemaphoreType.DMA((len(arrays),))],
        compiler_params=limit(4),
        cost_estimate=pl.CostEstimate(
            flops=4000000, bytes_accessed=8 * arrays[0].size, transcendentals=0
        ),
        name="assemble",
    )(*arrays)


def spread_heads(ref, value, offset, stride, seqs, heads, steps, size, t):
    for h in range(heads):
        tile, lane = divmod(h * size, 128)
        part = value[:, tile * 128 : (tile + 1) * 128]
        if lane:
            part = pltpu.roll(part, 128 - lane, 1)
        ref[pl.ds(offset + h * steps + t, seqs, stride=stride), :] = part


def put_rows(ref, start, count, value, stride=None):
    for m in range(ref.shape[0]):
        ref[m, pl.ds(start, count, stride=stride), :] = value[:, m * 128 : (m + 1) * 128]


def get_rows(ref, start, count, stride=None):
    return jnp.concatenate(
        [ref[m, pl.ds(start, count, stride=stride), :] for m in range(ref.shape[0])], 1
    )


def own_heads(product, masks, group, steps):
    tile = group * steps
    total = None
    for m, mask in enumerate(masks):
        part = jnp.where(mask, product[m * tile : (m + 1) * tile], 0.0)
        total = part if total is None else total + part
    shift = steps
    acc = total
    for _ in range(group - 1):
        acc = acc + pltpu.roll(total, shift, 0)
        shift += steps
    return acc


def early_kernel(steps, size, axes, count, *refs):
    inputs = 12 + count if count else 8
    own = 11 if count else 8
    sources, refs = refs[:inputs], refs[inputs:]
    outputs = 7 if count else 3
    outs, refs = refs[:outputs], refs[outputs:]
    out_ref, low_ref, const_ref = outs[:3]
    held, (kscr, pscr, uscr, gscr, sems) = refs[:own], refs[own:]
    k_ref, v_ref, b_ref, d_ref, a_ref, s0_ref = held[:6]
    base_ref, last_ref = held[6:8]
    seqs, _, width = s0_ref.shape
    views = list(sources[:8])
    if count:
        part = block_of(axes[1], held[8].shape[1])
        views += [ref.at[:, part] for ref in sources[8:11]]
    copies = fetch(views, held, sems)
    for copy in copies[:5]:
        copy.wait()
    heads = width // size
    group = 8 // steps
    ones = head_ones(width, size)
    masks = [head_mask(g * group, group, steps, width, size) for g in range(heads // group)]
    pick = jnp.where(
        lax.broadcasted_iota(jnp.int32, (heads, width), 0)
        == lax.broadcasted_iota(jnp.int32, (heads, width), 1) // size,
        1.0,
        0.0,
    )
    keys = [k_ref[:, t, :].astype(F32) for t in range(steps)]
    for t in range(steps):
        spread_heads(kscr, keys[t], 0, heads * steps, seqs, heads, steps, size, t)
    pairs = [(t, r) for t in range(steps) for r in range(t + 1)]
    sums = head_sum(jnp.concatenate([keys[t] * keys[r] for t, r in pairs], 0), ones)
    raw = {p: sums[i * seqs : (i + 1) * seqs] for i, p in enumerate(pairs)}
    inv = [lax.rsqrt(raw[t, t] + EPS) for t in range(steps)]

    copies[5].wait()
    if count:
        half = sources[-1].at[block_of(axes[0], outs[6].shape[0])]
        wide = sources[11].shape[1]
        targets = [outs[3].at[:, i * wide : (i + 1) * wide] for i in range(count)]
        copies += fetch(
            [half] + list(sources[11:-1]), [outs[6]] + targets, sems.at[pl.ds(11, count + 1)]
        )

    def read(s, carry):
        kb = kscr[pl.ds(s * heads * steps, heads * steps), :][:, :size].astype(BF16)
        seen = own_heads(dot(kb, s0_ref[s].astype(BF16)), masks, group, steps)
        put_rows(pscr, s * 8, 8, seen)
        return carry

    lax.fori_loop(0, seqs, read, 0, unroll=min(seqs, 32))
    highest = lax.Precision.HIGHEST
    cumul, solved = [], []
    for t in range(steps):
        live = jnp.where(a_ref[...] > t, 1.0, 0.0)
        log = dot(d_ref[t] * live, pick, ((0,), (0,)), highest)
        strength = dot(jax.nn.sigmoid(b_ref[t]) * live, pick, ((0,), (0,)), highest)
        cumul.append(log if t == 0 else cumul[-1] + log)
        seen = get_rows(pscr, t, seqs, 8) * inv[t]
        rest = v_ref[:, t, :].astype(F32) - jnp.exp(cumul[t]) * seen
        for r in range(t):
            rest = rest - jnp.exp(cumul[t] - cumul[r]) * (raw[t, r] * inv[t] * inv[r]) * solved[r]
        solved.append(strength * rest)
    for t in range(steps):
        add = jnp.exp(cumul[-1] - cumul[t]) * inv[t] * solved[t]
        for g in range(group):
            put_rows(uscr, g * steps + t, seqs, add, 8)
    gscr[...] = jnp.exp(cumul[-1])

    def write(s, carry):
        ub = get_rows(uscr, s * 8, 8)
        wide = jnp.concatenate([jnp.where(m, ub, 0.0) for m in masks], 0).astype(BF16)
        kb = kscr[pl.ds(s * heads * steps, heads * steps), :][:, :size].astype(BF16)
        new = gscr[pl.ds(s, 1), :] * s0_ref[s] + dot(kb, wide, ((0,), (0,)))
        out_ref[s] = new
        low_ref[s] = new.astype(BF16)
        return carry

    lax.fori_loop(0, seqs, write, 0, unroll=min(seqs, 32))
    for copy in copies[6:]:
        copy.wait()
    if count:
        outs[4][0:1, :] = held[8][...]
        total = None
        for i, ref in enumerate(held[9:11]):
            rows, every = outs[5].shape[0], ref.shape[0]
            row = lax.broadcasted_iota(jnp.int32, (rows, every), 0) - i * heads
            col = lax.broadcasted_iota(jnp.int32, (rows, every), 1)
            chosen = (row >= 0) & (row < heads) & (col == row + lax.axis_index(axes[2]) * heads)
            term = dot(chosen.astype(F32).astype(BF16), ref[...])
            total = term if total is None else total + term
        outs[5][...] = total.astype(BF16)
    entry = jnp.where(
        lax.broadcasted_iota(jnp.int32, (size, width), 0)
        == lax.broadcasted_iota(jnp.int32, (size, width), 1) % size,
        1.0,
        0.0,
    )
    const_ref[0:1, :] = dot(base_ref[...], pick, precision=highest)
    const_ref[1:2, :] = dot(last_ref[...], entry, precision=highest)


def early(axes, state, prev, decay_base, out_gain, shared):
    prev_keys, prev_values, prev_beta, prev_decay, accepted = prev
    seqs, size, width = state.shape
    steps = prev_keys.shape[1]
    heads = width // size
    arrays = (
        prev_keys,
        prev_values,
        jnp.transpose(prev_beta, (1, 2, 0)),
        jnp.transpose(prev_decay, (1, 2, 0)),
        accepted.reshape(1, -1),
        state,
        decay_base.reshape(1, -1),
        out_gain.reshape(1, -1),
    )
    held = [like(a) for a in arrays]
    shapes = [
        jax.ShapeDtypeStruct(state.shape, F32),
        jax.ShapeDtypeStruct(state.shape, BF16),
        jax.ShapeDtypeStruct((8, width), F32),
    ]
    count = 0
    if shared:
        in_gain, w_beta, w_decay, weights, w_out = shared
        count = len(weights)
        rows, columns = weights[0].shape
        arrays += (in_gain.reshape(1, -1), w_beta.T, w_decay.T) + weights + (w_out,)
        small = VMEM((w_beta.shape[1], rows), BF16)
        held += [VMEM((1, rows), F32), small, small]
        shapes += [
            jax.ShapeDtypeStruct((rows, columns * count), BF16),
            jax.ShapeDtypeStruct((8, rows), F32),
            jax.ShapeDtypeStruct((-(-2 * heads // 8) * 8, rows), BF16),
            jax.ShapeDtypeStruct((w_out.shape[0] // 2, w_out.shape[1]), BF16),
        ]
    return pl.pallas_call(
        functools.partial(early_kernel, steps, size, axes, count),
        out_shape=shapes,
        in_specs=[whole(HBM)] * len(arrays),
        out_specs=[whole()] * len(shapes),
        scratch_shapes=held
        + [
            VMEM((seqs * heads * steps, 128), F32),
            VMEM((width // 128, seqs * 8, 128), F32),
            VMEM((width // 128, seqs * 8, 128), F32),
            VMEM((seqs, width), F32),
            pltpu.SemaphoreType.DMA((len(arrays),)),
        ],
        cost_estimate=pl.CostEstimate(
            flops=seqs * 4000000, bytes_accessed=8 * state.size, transcendentals=0
        ),
        compiler_params=limit(20),
        name="early",
    )(*[pltpu.with_memory_space_constraint(a, HBM) for a in arrays])


def propose_kernel(dims, axis, spans, first, seqs, slot, const_ref, s_ref, *refs):
    steps, size, features = dims
    parts = len(spans)
    part_refs, wo, refs = refs[:parts], refs[parts], refs[parts + 1 :]
    stat_in = None if any(sums is not None for _, sums in spans) else refs[0]
    out_refs, (kscr, pscr) = refs[0 if stat_in is None else 1 : -2], refs[-2:]
    width = s_ref.shape[2]
    extra = -(-2 * (width // size) // 8) * 8
    heads = width // size
    group = 8 // steps
    ones = head_ones(width, size)
    masks = [head_mask(g * group, group, steps, width, size) for g in range(heads // group)]
    rows = seqs * steps

    def gathered(starts, count, lanes):
        total = None
        for ref, start in zip(part_refs, starts):
            if start is not None:
                piece = ref[start : start + count, lanes].astype(F32)
                total = piece if total is None else total + piece
        return total

    starts = [start for start, _ in spans]
    if stat_in is None:
        stat = gathered([sums for _, sums in spans], extra, slice(None))
        if slot is not None:
            out_refs[-1][...] = stat
            out_refs = out_refs[:-1]
    else:
        stat = stat_in[...]
    at_slot = 512 * (slot or 0)
    stat = stat[:, at_slot : at_slot + 512]
    logits = stat[:, :128] + stat[:, 128:256]
    total = stat[:, 256:384] + stat[:, 384:]
    flat = jnp.concatenate([logits, total], 0).T[:rows]
    src = lax.broadcasted_iota(jnp.int32, (2 * extra, width), 0)
    head = lax.broadcasted_iota(jnp.int32, (2 * extra, width), 1) // size
    highest = lax.Precision.HIGHEST
    base, gain = const_ref[0:1, :], const_ref[1:2, :]

    def take(row):
        return dot(flat, jnp.where(src == row, 1.0, 0.0), precision=highest)

    scale = lax.rsqrt(take(extra) / features + EPS)
    strength = jax.nn.sigmoid(scale * take(head))
    rate = scale * take(heads + head)
    log = -base * (jnp.maximum(rate, 0.0) + jnp.log1p(jnp.exp(-jnp.abs(rate))))

    def column(w):
        return gathered(starts, rows, slice(w * width, (w + 1) * width)) * scale

    query, key = column(0), column(1)
    squares = head_sum(jnp.concatenate([query * query, key * key], 0), ones)
    query = query * (lax.rsqrt(squares[:rows] + EPS) * size ** (-0.5))
    key = key * lax.rsqrt(squares[rows:] + EPS)

    def at(array, t):
        return array[t * seqs : (t + 1) * seqs]

    stride = 2 * heads * steps
    for t in range(steps):
        spread_heads(kscr, at(query, t), 0, stride, seqs, heads, steps, size, t)
        spread_heads(kscr, at(key, t), heads * steps, stride, seqs, heads, steps, size, t)
    below = [(t, r) for t in range(steps) for r in range(t)]
    inside = [(t, r) for t in range(steps) for r in range(t + 1)]
    products = [at(key, t) * at(key, r) for t, r in below]
    products += [at(query, t) * at(key, r) for t, r in inside]
    sums = head_sum(jnp.concatenate(products, 0), ones)
    k_k = {p: at(sums, i) for i, p in enumerate(below)}
    q_k = {p: at(sums, len(below) + i) for i, p in enumerate(inside)}
    upper = lax.broadcasted_iota(jnp.int32, (8, width), 0) < steps

    def read(s, carry):
        vectors = kscr[pl.ds(s * stride, stride), :][:, :size].astype(BF16)
        seen = dot(vectors, s_ref[first + s])
        half = heads * steps
        from_query = own_heads(seen[:half], masks, group, steps)
        from_key = own_heads(seen[half:], masks, group, steps)
        put_rows(pscr, s * 8, 8, jnp.where(upper, from_query, from_key))
        return carry

    lax.fori_loop(0, seqs, read, 0, unroll=seqs)
    value, gate = column(2), column(3)
    cumul, solved, outs = [], [], []
    for t in range(steps):
        cumul.append(at(log, t) if t == 0 else cumul[-1] + at(log, t))
        grown = jnp.exp(cumul[t])
        rest = at(value, t) - grown * get_rows(pscr, steps + t, seqs, 8)
        out = grown * get_rows(pscr, t, seqs, 8)
        for r in range(t):
            decay = jnp.exp(cumul[t] - cumul[r])
            rest = rest - decay * k_k[t, r] * solved[r]
            out = out + decay * q_k[t, r] * solved[r]
        solved.append(at(strength, t) * rest)
        outs.append(out + q_k[t, t] * solved[t])
    output = jnp.concatenate(outs, 0)
    mean = head_sum(output * output, ones) * (1.0 / size)
    gated = output * lax.rsqrt(mean + EPS) * gain * (gate / (1.0 + jnp.exp(-gate)))
    gated = gated.astype(BF16)
    n = wo.shape[0]
    tp = lax.axis_index(axis)
    for s in list(range(1, len(out_refs))) + [0]:
        block = wo[lax.bitwise_xor(tp, s)] if n > 1 else wo[0]
        out_refs[s][...] = dot(gated, block).astype(out_refs[s].dtype)


def propose(axis, consts, state, parts, spans, wo, dims, first, seqs, slot, stat):
    steps, size = dims[0], dims[1]
    width = state.shape[2]
    heads = width // size
    rows = seqs * steps
    shapes = [
        jax.ShapeDtypeStruct((rows, wo.shape[2]), F32 if s == 0 and wo.shape[0] > 1 else BF16)
        for s in range(wo.shape[0])
    ]
    inputs = [consts, state, *parts, wo]
    if stat is not None:
        inputs.append(stat)
    elif slot is not None:
        extra = -(-2 * heads // 8) * 8
        shapes.append(jax.ShapeDtypeStruct((extra, parts[0].shape[1]), F32))
    return pl.pallas_call(
        functools.partial(propose_kernel, dims, axis, spans, first, seqs, slot),
        out_shape=shapes,
        in_specs=[whole()] * len(inputs),
        out_specs=[whole()] * len(shapes),
        scratch_shapes=[
            VMEM((seqs * 2 * heads * steps, 128), F32),
            VMEM((width // 128, seqs * 8, 128), F32),
        ],
        compiler_params=limit(12),
        cost_estimate=pl.CostEstimate(
            flops=seqs * 4000000, bytes_accessed=4 * state.size, transcendentals=0
        ),
        name="propose",
    )(*inputs)


def finish_kernel(steps, chunks, *refs):
    ins, out_ref = refs[:-1], refs[-1]
    per = len(ins) // len(chunks)
    for c, (first, each) in enumerate(chunks):
        total = ins[c * per][...].astype(F32)
        for ref in ins[c * per + 1 : (c + 1) * per]:
            total = total + ref[...].astype(F32)
        for t in range(steps):
            out_ref[first : first + each, t, :] = total[t * each : (t + 1) * each].astype(
                out_ref.dtype
            )


def finish(pieces, chunks, seqs, steps):
    flat = [a for piece in pieces for a in piece]
    return pl.pallas_call(
        functools.partial(finish_kernel, steps, chunks),
        out_shape=jax.ShapeDtypeStruct((seqs, steps, flat[0].shape[1]), BF16),
        in_specs=[whole()] * len(flat),
        out_specs=whole(),
        compiler_params=limit(8),
        name="finish",
    )(*flat)


def split(seqs):
    last = max(8, seqs // 4)
    return ((0, seqs - last), (seqs - last, last)) if seqs % 8 == 0 and seqs > 8 else ((0, seqs),)


def body(sizes, *args):
    return layer(sizes, *args)


def layer(
    sizes,
    tokens,
    in_gain,
    w_query,
    w_key,
    w_value,
    w_gate,
    w_beta,
    w_decay,
    decay_base,
    out_gain,
    w_out,
    state,
    prev_keys,
    prev_values,
    prev_beta,
    prev_decay,
    accepted,
):
    n_grp, n_kv, n_tp = sizes
    seqs, steps, _ = tokens.shape
    heads = decay_base.shape[0]
    size = out_gain.shape[0]
    features = in_gain.shape[0]
    dims = (steps, size, features)
    square = n_kv == n_tp and n_kv & (n_kv - 1) == 0 and n_grp == 2
    chunks = split(seqs) if square else ((0, seqs),)
    axes = ("grp", "kv", "tp")
    weights = (w_query, w_key, w_value, w_gate)
    prev = (prev_keys, prev_values, prev_beta, prev_decay, accepted)

    def ring(n, s):
        return [(i, (i + s) % n) for i in range(n)]

    if square:
        n = n_kv
        bits = [n >> i for i in range(1, n.bit_length())]
        turn = [(k * n + t, t * n + (k ^ t)) for k in range(n) for t in range(n)]
        turned = lax.ppermute(tokens, ("kv", "tp"), turn)
    shared = (in_gain, w_beta, w_decay, weights, w_out) if square else None
    new_state, low, consts, *staged = early(axes, state, prev, decay_base, out_gain, shared)
    if square:
        weight, own_gain, small, mine = staged
        turned, weight = lax.optimization_barrier((turned, weight))
        halves, marks = [mine], [0]

        def swap(array, bit):
            return lax.ppermute(array, "kv", [(i, i ^ bit) for i in range(n)])

        halves.append(swap(mine, bits[0]))
        marks.append(bits[0])
        halves.append(swap(mine, bits[1]))
        marks.append(bits[1])
        gathered = lax.all_gather(turned, "tp")
        parts = [[None] * n for _ in chunks]
        rest = [i for i in range(n) if i != bits[0]]
        for owners in ([bits[0]], rest):
            layout = [
                (i, (c,), c == 0, F32 if i == 0 else BF16)
                for c in range(len(chunks))
                for i in owners
            ]
            products = project(gathered, own_gain, weight, small, chunks, layout)
            for (i, (c,), _, _), product in zip(layout, products):
                parts[c][i] = product
        spans = []
        for c, (first, each) in enumerate(chunks):
            for i in range(1, n):
                parts[c][i] = swap(parts[c][i], i)
            spans.append([(0, each * steps if c == 0 else None)] * n)
        halves, parts[0][0] = lax.optimization_barrier((halves, parts[0][0]))
        for bit in bits[1:]:
            for j in range(len(halves)):
                if marks[j] ^ bit not in marks:
                    halves.append(swap(halves[j], bit))
                    marks.append(marks[j] ^ bit)
        arrays, blocks = [w_out], [(0, None)]
        for i in range(1, len(halves)):
            other = lax.ppermute(halves[i], "grp", ring(n_grp, 1))
            arrays += [halves[i], other]
            blocks += [(marks[i], 0), (marks[i], 1)]
        wo = assemble(axes, arrays, blocks, n)
    else:
        x = lax.all_gather(tokens, "tp", axis=2, tiled=True)
        x = jnp.transpose(x, (1, 0, 2)).reshape(seqs * steps, -1).astype(F32)
        square_sum = jnp.sum(x * x, -1)
        x = (x * in_gain).astype(BF16)
        full = [lax.all_gather(w, "kv", axis=0, tiled=True) for w in weights]
        products = [jnp.dot(x, w, preferred_element_type=F32) for w in full]
        start = lax.axis_index("tp") * heads
        chosen = [lax.dynamic_slice_in_dim(w, start, heads, 1) for w in (w_beta, w_decay)]
        logits = jnp.dot(x, jnp.concatenate(chosen, 1), preferred_element_type=F32).T
        extra = -(-2 * heads // 8) * 8
        sums = jnp.zeros((extra, sum(p.shape[1] for p in products)), F32)
        sums = sums.at[: 2 * heads, : seqs * steps].set(logits)
        sums = sums.at[0, 256 : 256 + seqs * steps].set(square_sum)
        parts = [[jnp.concatenate([jnp.concatenate(products, 1), sums], 0)]]
        spans = [[(0, seqs * steps)]]
        wo = lax.all_gather(w_out, "kv", axis=1, tiled=True)[None]

    pieces, stat = [], None
    for c, (first, each) in enumerate(chunks):
        slot = c if len(chunks) > 1 else None
        out = propose(
            "tp", consts, low, parts[c], spans[c], wo, dims, first, each, slot, stat
        )
        if slot == 0:
            stat = out[-1]
        if square:
            pieces.append(
                [out[0]]
                + [
                    lax.ppermute(out[s], "tp", [(i, i ^ s) for i in range(n_tp)])
                    for s in range(1, n_tp)
                ]
            )
        else:
            pieces.append([lax.psum_scatter(out[0], "tp", scatter_dimension=1, tiled=True)])
    return finish(pieces, chunks, seqs, steps), new_state


def solution(mesh):
    rows = P(("grp", "kv"), None, "tp")
    matrix = P("kv", "tp")
    placed = (
        rows,
        P(),
        matrix,
        matrix,
        matrix,
        matrix,
        P(),
        P(),
        P("tp"),
        P(),
        P("tp", "kv"),
        rows,
        rows,
        rows,
        rows,
        rows,
        P(("grp", "kv")),
    )
    sizes = (mesh.shape["grp"], mesh.shape["kv"], mesh.shape["tp"])
    return jax.shard_map(
        functools.partial(body, sizes),
        mesh=mesh,
        in_specs=placed,
        out_specs=(rows, rows),
        check_vma=False,
    )
```
